32 devices in a mesh: ep: 8 (over z, x), tp: 4 (over y, core).
Axes of the slice: x: 2, y: 2, z: 4, core: 2. Of those that a mesh axis runs over, the one named last changes fastest.
Arguments:
- query_latent: bfloat16 [4096, 768], P(('ep', 'tp')), may hold values from -6 to 6
- kv_latent: bfloat16 [4096, 512], P(('ep', 'tp')), may hold values from -6 to 6
- rope_key: bfloat16 [4096, 64], P(('ep', 'tp')), may hold values from -6 to 6
- query_gain: float32 [768], replicated, may hold values from 0.1 to 12
- kv_gain: float32 [512], replicated, may hold values from 0.1 to 12
- query_nope_w: bfloat16 [768, 1024], P(None, 'tp'), may hold values from -0.21875 to 0.21875
- query_rope_w: bfloat16 [768, 512], P(None, 'tp'), may hold values from -0.21875 to 0.21875
- key_up_w: bfloat16 [512, 1024], P(None, 'tp'), may hold values from -0.25 to 0.25
- value_up_w: bfloat16 [512, 1024], P(None, 'tp'), may hold values from -0.25 to 0.25
- output_w: bfloat16 [1024, 2048], P('tp'), may hold values from -0.1875 to 0.1875
- expert_in: bfloat16 [4096, 2048], P(('ep', 'tp')), may hold values from -6 to 6
- moe_gain: float32 [2048], replicated, may hold values from 0.1 to 12
- routes: int32 [4096, 2], P(('ep', 'tp')), may hold values from 0 to 15, all different within a row; in each aligned block of 128 rows (0 to 127, 128 to 255, ...) at most 20 rows name the same one
- route_weight: float32 [4096, 2], P(('ep', 'tp')), may hold values from 0.1 to 1
- gate_w: bfloat16 [16, 2048, 2048], P('ep', None, 'tp'), may hold values from -0.125 to 0.125
- up_w: bfloat16 [16, 2048, 2048], P('ep', None, 'tp'), may hold values from -0.125 to 0.125
- down_w: bfloat16 [16, 2048, 2048], P('ep', 'tp'), may hold values from -0.125 to 0.125
Outputs:
- mixer_out: bfloat16 [4096, 2048], P(('ep', 'tp'))
- expert_out: bfloat16 [4096, 2048], P(('ep', 'tp'))
The draws below stay inside these ranges and needn't reach their ends.
Inputs may be any that keep to these rules, and one draw needn't show every extreme that they name: `routes`: each row names 2 different experts; in the rows of one device no expert is named more than 20 times.
All inputs are finite; a program needn't handle non-finite values.
Results may differ from the reference program's by a relative error of at most 0.015.
The reference program's roundings to bfloat16 on the way count: a program that leaves them out, or rounds other values in their place, can miss the bound.
Values may be sent and summed in bfloat16 or wider, within the bound.
A program may use at most 128 MiB of HBM per device.

```python
import math
import jax
import jax.numpy as jnp
import numpy as np
from jax import lax

D = 2048
HEADS = 8
NOPE = 128
ROPE = 64
VDIM = 128
QLAT = 768
KVLAT = 512
FF = 2048
TOPK = 2
TOK_B = 128
EXPERTS = 16
CAP = 20
TOKENS_A = 4096
TOKENS_B = 4096
N_EP = 8
N_TP = 4


def gain_draw(key, count):
    return 1.0 + 0.18 * jnp.clip(jax.random.normal(key, (count,), jnp.float32), -5.0, 5.0)


def draw_query_gain(key, part):
    return gain_draw(jax.random.fold_in(key, 11), QLAT)


def draw_kv_gain(key, part):
    return gain_draw(jax.random.fold_in(key, 23), KVLAT)


def draw_moe_gain(key, part):
    return gain_draw(jax.random.fold_in(key, 37), D)


def levels(rng, dims, shards, low, top_value):
    loudness, own = 1.0, jax.random.fold_in(rng, 6)
    for position, blocks in shards:
        heights = jnp.exp(jax.random.uniform(jax.random.fold_in(own, position), (blocks,), jnp.float32, low / len(shards), top_value / len(shards)))
        loudness = loudness * jnp.repeat(heights, dims[position] // blocks).reshape([-1 if axis == position else 1 for axis in range(len(dims))])
    return loudness


def assign_block(own_key, own, number, rows, number_of, top, bound, skew):
    ranking = jax.random.permutation(own_key, number_of)
    packed, common = load_shares(number_of, rows * top, bound, skew, True), load_shares(number_of, rows * top, bound, skew, False)
    places = jnp.arange(number_of)

    def named(lengths, offset_by):
        used = int((lengths > 0).sum())
        fixed = max(1, used // 4)
        shifted = fixed + (places - fixed + offset_by * (used - fixed)) % max(1, number_of - fixed)
        return jnp.zeros((number_of,), jnp.int32).at[ranking[jnp.where(places < fixed, places, shifted)]].set(jnp.asarray(lengths, jnp.int32))

    lengths = jnp.where(number % 4 == 0, named(packed, number // 4), named(common, number - number // 4 - 1))
    mixed = jax.random.permutation(jax.random.fold_in(own, 3), number_of)
    donor, receiver = mixed[0:number_of // 2 * 2:2], mixed[1:number_of // 2 * 2:2]
    room = jnp.minimum(lengths[donor] - 1, bound - lengths[receiver]) // 2
    room = jnp.where((donor == ranking[0]) | (receiver == ranking[0]) | (lengths[receiver] == 0), 0, jnp.maximum(room, 0))
    shifted = jax.random.randint(jax.random.fold_in(own, 4), (number_of // 2,), 0, 1 << 20) % (room + 1)
    lengths = lengths.at[donor].add(-shifted).at[receiver].add(shifted)
    members = jnp.searchsorted(jnp.cumsum(lengths), jnp.arange(rows * top), side="right").astype(jnp.int32)
    listing = members.reshape(top, rows).T
    listing = listing[jax.random.permutation(jax.random.fold_in(own, 1), rows)]
    offset_by = jax.random.randint(jax.random.fold_in(own, 2), (rows, 1), 0, top)
    return jnp.take_along_axis(listing, (jnp.arange(top)[None, :] + offset_by) % top, axis=1)


def load_shares(count, total, bound, slope, full):
    weights = [(1 << 20) // math.isqrt(rank ** slope) + 1 for rank in range(1, count + 1)]
    largest = bound if full else min(bound, max(-(-total // count), total * weights[0] // sum(weights)))
    least = 1 if total - largest >= count - 1 else 0
    given, surplus = [largest] + [least] * (count - 1), total - largest - least * (count - 1)
    while surplus > 0:
        candidates = [i for i in range(1, count) if given[i] < largest] or [i for i in range(1, count) if given[i] < bound]
        pool, budget = sum([weights[i] for i in candidates]), surplus
        for i in candidates:
            extra = min(bound - given[i], max(1, budget * weights[i] // pool), surplus)
            given[i] = given[i] + extra
            surplus = surplus - extra
    return np.array(given)


def noise(stream_key, shape, scale, reach, shards=(), kind=jnp.bfloat16):
    entries = scale * jax.random.normal(stream_key, shape, jnp.float32)
    if shards:
        entries = entries * levels(stream_key, shape, shards, -0.22, 0.18)
    return jnp.clip(entries, -reach, reach).astype(kind)


def setup_inputs(seed: int = 0) -> dict:
    key_list = jax.random.split(jax.random.key(seed), 18)
    query_latent = noise(key_list[0], (TOKENS_A, QLAT), 1.0, 6.0, ((0, 32),))
    kv_latent = noise(key_list[1], (TOKENS_A, KVLAT), 1.0, 6.0, ((0, 32),))
    rope_key = noise(key_list[2], (TOKENS_A, ROPE), 1.0, 6.0, ((0, 32),))
    query_gain = draw_query_gain(jax.random.fold_in(key_list[17], 71), 0)
    kv_gain = draw_kv_gain(jax.random.fold_in(key_list[17], 71), 0)
    query_nope_w = noise(key_list[5], (QLAT, HEADS * NOPE), QLAT ** -0.5, 0.21875, ((1, 4),))
    query_rope_w = noise(key_list[6], (QLAT, HEADS * ROPE), QLAT ** -0.5, 0.21875, ((1, 4),))
    key_up_w = noise(key_list[7], (KVLAT, HEADS * NOPE), KVLAT ** -0.5, 0.25, ((1, 4),))
    value_up_w = noise(key_list[8], (KVLAT, HEADS * VDIM), KVLAT ** -0.5, 0.25, ((1, 4),))
    output_w = noise(key_list[9], (HEADS * VDIM, D), (HEADS * VDIM) ** -0.5, 0.1875, ((0, 4),))
    expert_in = noise(key_list[10], (TOKENS_B, D), 1.0, 6.0, ((0, 32),))
    moe_gain = draw_moe_gain(jax.random.fold_in(key_list[17], 71), 0)
    routes_keys = jax.random.split(jax.random.fold_in(key_list[12], 1), TOKENS_B // TOK_B)
    routes_turns = jax.random.permutation(jax.random.fold_in(key_list[12], 3), TOKENS_B // TOK_B)
    routes = jax.vmap(lambda own, number: assign_block(jax.random.fold_in(key_list[12], 2), own, number, TOK_B, EXPERTS, TOPK, CAP, 1))(routes_keys, routes_turns).reshape((TOKENS_B, TOPK))
    route_weight = jnp.clip(jnp.exp(math.log(1.0) - 2.3025851 * jax.random.uniform(key_list[13], (TOKENS_B, TOPK), jnp.float32) ** levels(key_list[13], (TOKENS_B, TOPK), ((0, 32),), -0.2, 0.2)), 0.1, 1.0)
    gate_w = noise(key_list[14], (EXPERTS, D, FF), D ** -0.5, 0.125, ((0, 8), (2, 4)))
    up_w = noise(key_list[15], (EXPERTS, D, FF), D ** -0.5, 0.125, ((0, 8), (2, 4)))
    down_w = noise(key_list[16], (EXPERTS, FF, D), FF ** -0.5, 0.125, ((0, 8), (1, 4)))
    return dict(query_latent=query_latent, kv_latent=kv_latent, rope_key=rope_key, query_gain=query_gain, kv_gain=kv_gain, query_nope_w=query_nope_w, query_rope_w=query_rope_w, key_up_w=key_up_w, value_up_w=value_up_w, output_w=output_w, expert_in=expert_in, moe_gain=moe_gain, routes=routes, route_weight=route_weight, gate_w=gate_w, up_w=up_w, down_w=down_w)


THETA = 10000.0

def rms_scale(values, gain):
    floats = values.astype(jnp.float32)
    square = lax.optimization_barrier(jnp.mean(floats * floats, axis=-1, keepdims=True))
    return (floats * lax.rsqrt(square + 1e-06) * gain).astype(jnp.bfloat16)

def rotate(values, positions):
    width = values.shape[-1]
    half = width // 2
    freq = 1.0 / THETA ** (jnp.arange(half, dtype=jnp.float32) * 2.0 / width)
    angle = positions.astype(jnp.float32)[:, None] * freq[None, :]
    angle = jnp.concatenate([angle, angle], axis=-1)
    cosine = jnp.cos(angle)
    sine = jnp.sin(angle)
    if values.ndim == 3:
        cosine = cosine[:, None, :]
        sine = sine[:, None, :]
    first = values[..., :half]
    second = values[..., half:]
    turned = jnp.concatenate([-second, first], axis=-1)
    return values * cosine + turned * sine

def expert_rows(rows, gate_one, up_one, down_one):
    gate = jnp.minimum(jnp.dot(rows, gate_one, preferred_element_type=jnp.float32), 7.0)
    upper = jnp.clip(jnp.dot(rows, up_one, preferred_element_type=jnp.float32), -7.0, 7.0)
    hidden = (gate * jax.nn.sigmoid(1.702 * gate) * (upper + 1.0)).astype(jnp.bfloat16)
    count = rows.shape[0]
    slices = hidden.reshape(count, N_TP, FF // N_TP).astype(jnp.float32)
    downs = down_one.reshape(N_TP, FF // N_TP, D).astype(jnp.float32)
    parts = jnp.einsum('rsf,sfd->srd', slices, downs)
    parts = lax.optimization_barrier(parts.astype(jnp.bfloat16)).astype(jnp.float32)
    return lax.optimization_barrier(jnp.sum(parts, axis=0)).astype(jnp.bfloat16)

def reference(query_latent, kv_latent, rope_key, query_gain, kv_gain, query_nope_w, query_rope_w, key_up_w, value_up_w, output_w, expert_in, moe_gain, routes, route_weight, gate_w, up_w, down_w):
    length = query_latent.shape[0]
    positions = jnp.arange(length, dtype=jnp.int32)
    query_normed = rms_scale(query_latent, query_gain)
    kv_normed = rms_scale(kv_latent, kv_gain)
    query_flat = jnp.dot(query_normed, query_nope_w, preferred_element_type=jnp.float32).astype(jnp.bfloat16)
    key_flat = jnp.dot(kv_normed, key_up_w, preferred_element_type=jnp.float32).astype(jnp.bfloat16)
    value_flat = jnp.dot(kv_normed, value_up_w, preferred_element_type=jnp.float32).astype(jnp.bfloat16)
    query_turn = jnp.dot(query_normed, query_rope_w, preferred_element_type=jnp.float32).reshape(length, HEADS, ROPE)
    query_rot = rotate(query_turn, positions).astype(jnp.bfloat16)
    key_rot = rotate(rope_key.astype(jnp.float32), positions).astype(jnp.bfloat16)
    queries = jnp.concatenate([query_flat.reshape(length, HEADS, NOPE), query_rot], axis=-1).astype(jnp.float32)
    keys = jnp.concatenate([key_flat.reshape(length, HEADS, NOPE), jnp.broadcast_to(key_rot[:, None, :], (length, HEADS, ROPE))], axis=-1).astype(jnp.float32)
    values = value_flat.reshape(length, HEADS, VDIM).astype(jnp.float32)
    block = math.gcd(length, 512)
    scale = 1.0 / math.sqrt(NOPE + ROPE)

    def attend(start):
        query_block = lax.dynamic_slice_in_dim(queries, start, block, 0)
        scores = jnp.einsum('qhd,khd->hqk', query_block, keys) * scale
        allowed = positions[None, :] <= (start + jnp.arange(block, dtype=jnp.int32))[:, None]
        masked = jnp.where(allowed[None], scores, -1e+30)
        peak = lax.optimization_barrier(jnp.max(masked, axis=-1, keepdims=True))
        expo = jnp.where(allowed[None], jnp.exp(masked - peak), 0.0)
        total = lax.optimization_barrier(jnp.sum(expo, axis=-1))
        probs = expo.astype(jnp.bfloat16).astype(jnp.float32)
        summed = jnp.einsum('hqk,khd->qhd', probs, values)
        return (summed / jnp.transpose(total)[:, :, None]).astype(jnp.bfloat16)
    starts = jnp.arange(length // block, dtype=jnp.int32) * block
    attended = lax.map(attend, starts).reshape(length, HEADS * VDIM)
    group = HEADS * VDIM // N_TP
    mixed = jnp.zeros((length, D), jnp.float32)
    for index in range(N_TP):
        part = jnp.dot(attended[:, index * group:(index + 1) * group], output_w[index * group:(index + 1) * group], preferred_element_type=jnp.float32)
        mixed = mixed + lax.optimization_barrier(part.astype(jnp.bfloat16)).astype(jnp.float32)
    mixer_out = mixed.astype(jnp.bfloat16)
    floats = expert_in.astype(jnp.float32)
    center = floats - lax.optimization_barrier(jnp.mean(floats, axis=-1, keepdims=True))
    variance = lax.optimization_barrier(jnp.mean(center * center, axis=-1, keepdims=True))
    normed_in = (center * lax.rsqrt(variance + 1e-05) * moe_gain).astype(jnp.bfloat16)
    tokens_b = expert_in.shape[0]
    flat = routes.reshape(-1).astype(jnp.int32)
    assigned = flat.shape[0]
    owner = (jnp.arange(assigned, dtype=jnp.int32) // TOPK).astype(jnp.int32)
    weights = route_weight / lax.optimization_barrier(jnp.sum(route_weight, axis=-1, keepdims=True))
    flat_weight = weights.reshape(-1)
    order = jnp.argsort(flat, stable=True).astype(jnp.int32)
    counts = lax.optimization_barrier(jnp.sum((flat[:, None] == jnp.arange(EXPERTS, dtype=jnp.int32)[None, :]).astype(jnp.int32), axis=0))
    firsts = (jnp.cumsum(counts) - counts).astype(jnp.int32)
    most_rows = N_EP * N_TP * CAP

    def per_expert(total, expert):
        offsets = jnp.arange(most_rows, dtype=jnp.int32)
        valid = offsets < counts[expert]
        index = jnp.minimum(firsts[expert] + offsets, assigned - 1).astype(jnp.int32)
        picked = order[index]
        rows = normed_in[owner[picked]]
        result = expert_rows(rows, gate_w[expert], up_w[expert], down_w[expert])
        factor = jnp.where(valid, flat_weight[picked], 0.0)
        total = total.at[owner[picked]].add(factor[:, None] * result.astype(jnp.float32))
        return (total, None)
    combined, unused = lax.scan(per_expert, jnp.zeros((tokens_b, D), jnp.float32), jnp.arange(EXPERTS, dtype=jnp.int32))
    return (mixer_out, combined.astype(jnp.bfloat16))
```

```python
import functools
import math

import jax
import jax.numpy as jnp
from jax import lax
from jax.experimental import pallas as pl
from jax.experimental.pallas import tpu as pltpu
from jax.sharding import PartitionSpec as P

NOPE = 128


THETA = 10000.0

PAD = 256

NT = (((1,), (1,)), ((), ()))


def rms_scale(values, gain):
    floats = values.astype(jnp.float32)
    square = jnp.mean(floats * floats, axis=-1, keepdims=True)
    return (floats * lax.rsqrt(square + 1e-06) * gain).astype(jnp.bfloat16)


def attend_kernel(heads, rope, last_ref, lat_ref, q_ref, wk_ref, wv_ref, out_ref, peak, total, acc):
    rows = q_ref.shape[0]
    vdim = wv_ref.shape[0] // heads
    scale = math.log2(math.e) / math.sqrt(NOPE + rope)
    peak[...] = jnp.full_like(peak, -1e30)
    total[...] = jnp.zeros_like(total)
    acc[...] = jnp.zeros_like(acc)

    def block(number, masked):
        lat = lat_ref[pl.ds(pl.multiple_of(number * rows, rows), rows), :]
        keys = jnp.dot(lat, wk_ref[...], preferred_element_type=jnp.float32).astype(jnp.bfloat16)
        vals = lax.dot_general(
            wv_ref[...], lat, NT, preferred_element_type=jnp.float32
        ).astype(jnp.bfloat16)
        for h in range(heads):
            score = (
                lax.dot_general(
                    keys[:, h * PAD : (h + 1) * PAD],
                    q_ref[:, h * PAD : (h + 1) * PAD],
                    NT,
                    preferred_element_type=jnp.float32,
                )
                * scale
            )
            if masked:
                key = lax.broadcasted_iota(jnp.int32, score.shape, 0)
                query = lax.broadcasted_iota(jnp.int32, score.shape, 1)
                score = jnp.where(key <= query, score, -1e30)
            old = peak[h : h + 1, :]
            new = jnp.maximum(old, jnp.max(score, axis=0, keepdims=True))
            expo = jnp.exp2(score - new)
            factor = jnp.exp2(old - new)
            peak[h : h + 1, :] = new
            total[h : h + 1, :] = total[h : h + 1, :] * factor + jnp.sum(
                expo, axis=0, keepdims=True
            )
            part = slice(h * vdim, (h + 1) * vdim)
            acc[part, :] = acc[part, :] * factor + jnp.dot(
                vals[part, :], expo.astype(jnp.bfloat16), preferred_element_type=jnp.float32
            )

    last = last_ref[0]

    @pl.loop(0, last)
    def _(number):
        block(number, False)

    block(last, True)
    for h in range(heads):
        part = slice(h * vdim, (h + 1) * vdim)
        out_ref[part, :] = (acc[part, :] / total[h : h + 1, :]).astype(jnp.bfloat16)


def attend(last, latents, queries, key_w, value_w, heads, rope):
    rows = queries.shape[0]
    vdim_all = value_w.shape[0]
    vmem = pl.BlockSpec(memory_space=pltpu.VMEM)
    length = latents.shape[0]
    return pl.pallas_call(
        functools.partial(attend_kernel, heads, rope),
        out_shape=jax.ShapeDtypeStruct((vdim_all, rows), jnp.bfloat16),
        in_specs=[pl.BlockSpec(memory_space=pltpu.SMEM)] + [vmem] * 4,
        out_specs=vmem,
        scratch_shapes=[
            pltpu.VMEM((heads, rows), jnp.float32),
            pltpu.VMEM((heads, rows), jnp.float32),
            pltpu.VMEM((vdim_all, rows), jnp.float32),
        ],
        compiler_params=pltpu.CompilerParams(vmem_limit_bytes=40 * 1024 * 1024),
        cost_estimate=pl.CostEstimate(
            flops=2 * length * rows * heads * (PAD + 2 * NOPE),
            bytes_accessed=latents.size * 2,
            transcendentals=length * rows * heads,
        ),
    )(last, latents, queries, key_w, value_w)


def mixer_front(query_latent, kv_latent, rope_key, query_gain, kv_gain):
    tok_rows = query_latent.shape[0]
    rope = rope_key.shape[1]
    half = rope // 2
    group_rows = tok_rows * lax.axis_size("tp")
    freq = 1.0 / THETA ** (jnp.arange(half, dtype=jnp.float32) * 2.0 / rope)
    first_pos = lax.axis_index("ep") * group_rows
    positions = first_pos + jnp.arange(group_rows, dtype=jnp.int32)
    own = lax.axis_index("tp") * tok_rows + first_pos + jnp.arange(tok_rows, dtype=jnp.int32)
    angle = own.astype(jnp.float32)[:, None] * jnp.tile(freq, 2)[None, :]
    keys = rope_key.astype(jnp.float32)
    turned = jnp.concatenate([-keys[:, half:], keys[:, :half]], axis=-1)
    key_rot = (keys * jnp.cos(angle) + turned * jnp.sin(angle)).astype(jnp.bfloat16)
    kv_normed = rms_scale(kv_latent, kv_gain)
    own_latents = jnp.concatenate([kv_normed, key_rot], axis=1)
    query_normed = lax.all_gather(rms_scale(query_latent, query_gain), "tp", axis=0, tiled=True)
    return own_latents, query_normed, positions, freq


def mixer(
    front, rope, query_nope_w, query_rope_w, key_up_w, value_up_w, output_w
):
    latents, query_normed, positions, freq = front
    half = rope // 2
    heads = query_nope_w.shape[1] // NOPE
    kv_width = key_up_w.shape[0]
    angle = positions.astype(jnp.float32)[:, None] * jnp.tile(freq, 2 * heads)[None, :]
    turned_w = []
    for h in range(heads):
        turned_w.append(-query_rope_w[:, h * rope + half : (h + 1) * rope])
        turned_w.append(query_rope_w[:, h * rope : h * rope + half])
    weights = jnp.concatenate([query_nope_w, query_rope_w] + turned_w, axis=1)
    flat = jnp.dot(query_normed, weights, preferred_element_type=jnp.float32)
    nope_all = heads * NOPE
    rope_all = heads * rope
    rot = (
        flat[:, nope_all : nope_all + rope_all] * jnp.cos(angle)
        + flat[:, nope_all + rope_all :] * jnp.sin(angle)
    ).astype(jnp.bfloat16)
    query_flat = flat[:, :nope_all].astype(jnp.bfloat16)
    blank = jnp.zeros((flat.shape[0], PAD - NOPE - rope), jnp.bfloat16)
    pieces = []
    for h in range(heads):
        pieces += [
            query_flat[:, h * NOPE : (h + 1) * NOPE],
            rot[:, h * rope : (h + 1) * rope],
            blank,
        ]
    queries = jnp.concatenate(pieces, axis=1)
    carry = jnp.pad(
        jnp.eye(rope, dtype=jnp.bfloat16), ((0, 0), (NOPE, PAD - NOPE - rope))
    )
    key_w = jnp.concatenate(
        [
            jnp.concatenate(
                [
                    jnp.pad(key_up_w[:, h * NOPE : (h + 1) * NOPE], ((0, 0), (0, PAD - NOPE))),
                    carry,
                ],
                axis=0,
            )
            for h in range(heads)
        ],
        axis=1,
    )
    value_w = jnp.pad(value_up_w.T, ((0, 0), (0, latents.shape[1] - kv_width)))
    last = lax.axis_index("ep").astype(jnp.int32).reshape(1)
    attended = attend(last, latents, queries, key_w, value_w, heads, rope)
    mixed = lax.dot_general(
        attended, output_w, (((0,), (0,)), ((), ())), preferred_element_type=jnp.float32
    ).astype(jnp.bfloat16)
    return lax.psum_scatter(mixed, "tp", scatter_dimension=0, tiled=True)


def route(routes, experts, local, capacity):
    rows = routes.shape[0]
    main = capacity // 8 * 8
    rest = capacity - main
    names = jnp.arange(experts, dtype=jnp.int32)[None, :]
    chosen = [routes[:, k : k + 1] == names for k in range(routes.shape[1])]
    member = functools.reduce(jnp.logical_or, chosen).astype(jnp.bfloat16)
    before = lax.broadcasted_iota(jnp.int32, (rows, rows), 0) > lax.broadcasted_iota(
        jnp.int32, (rows, rows), 1
    )
    rank = jnp.dot(
        before.astype(jnp.bfloat16), member, preferred_element_type=jnp.float32
    ).astype(jnp.int32)
    inner = names % local
    place = jnp.where(
        rank < main, inner * main + rank, local * main + inner * rest + rank - main
    ) + names // local * (local * capacity)
    slots = lax.broadcasted_iota(jnp.int32, (rows, experts * capacity), 1)
    return [
        jnp.sum(jnp.where(one, place, 0), axis=1, keepdims=True) == slots for one in chosen
    ]


def swap(values, bit):
    size = lax.axis_size("tp")
    return lax.ppermute(values, "tp", [(one, one ^ bit) for one in range(size)])


def expert_rows(pieces, local, main, rest, gate_w, up_w, down_w):
    groups, piece, width = pieces.shape
    mixed = pieces[:, local * main :].reshape(groups * local * rest, width)
    owner = (
        lax.broadcasted_iota(jnp.int32, (groups * local * rest, 1), 0) % (local * rest)
    ) // max(rest, 1)
    mains = []
    shared = 0.0
    for expert in range(local):
        inputs = jnp.concatenate(
            [
                pieces[:, expert * main : (expert + 1) * main].reshape(groups * main, width),
                mixed,
            ],
            axis=0,
        )
        gate = jnp.minimum(jnp.dot(inputs, gate_w[expert], preferred_element_type=jnp.float32), 7.0)
        upper = jnp.clip(
            jnp.dot(inputs, up_w[expert], preferred_element_type=jnp.float32), -7.0, 7.0
        )
        hidden = (gate * jax.nn.sigmoid(1.702 * gate) * (upper + 1.0)).astype(jnp.bfloat16)
        output = jnp.dot(hidden, down_w[expert], preferred_element_type=jnp.float32).astype(
            jnp.bfloat16
        )
        mains.append(output[: groups * main].reshape(groups, main, width))
        shared = jnp.where(owner == expert, output[groups * main :], shared)
    shared = shared.astype(jnp.bfloat16).reshape(groups, local * rest, width)
    return jnp.concatenate(mains + [shared], axis=1)


def add_rounded(one, other):
    return (one.astype(jnp.float32) + other.astype(jnp.float32)).astype(jnp.bfloat16)


def group_experts(arrived, run):
    size = lax.axis_size("tp")
    if size & (size - 1):
        spread = lax.all_gather(arrived, "tp", axis=0, tiled=True)
        return lax.psum_scatter(run(spread), "tp", scatter_dimension=0, tiled=True)
    count = arrived.shape[0]
    far = {0: arrived}
    for bit in [1 << k for k in range(1, size.bit_length() - 1)]:
        for key in sorted(far):
            far[key | bit] = swap(far[key], bit)
    results = {}
    for key in sorted(far):
        if size == 1:
            results[key] = run(far[key])
            continue
        near = swap(far[key], 1)
        both = run(jnp.concatenate([far[key], near], axis=0))
        results[key] = add_rounded(both[:count], swap(both[count:], 1))
    for bit in [1 << k for k in range(size.bit_length() - 2, 0, -1)]:
        for key in sorted(results):
            if key & bit:
                results[key ^ bit] = add_rounded(results[key ^ bit], swap(results.pop(key), bit))
    return results[0]


def experts_half(expert_in, moe_gain, routes, route_weight, gate_w, up_w, down_w, tied):
    tok_rows, top_count = routes.shape
    width = expert_in.shape[1]
    local = gate_w.shape[0]
    ep_size = lax.axis_size("ep")
    experts = local * ep_size
    capacity = max(2, 5 * tok_rows * top_count // (4 * experts))
    main = capacity // 8 * 8
    rest = capacity - main
    piece = local * capacity
    floats = expert_in.astype(jnp.float32)
    center = floats - jnp.mean(floats, axis=-1, keepdims=True)
    variance = jnp.mean(center * center, axis=-1, keepdims=True)
    normed_in = (center * lax.rsqrt(variance + 1e-05) * moe_gain).astype(jnp.bfloat16)
    hits = route(routes, experts, local, capacity)
    select = functools.reduce(jnp.logical_or, hits).astype(jnp.bfloat16)
    outgoing = lax.dot_general(
        select, normed_in, (((0,), (0,)), ((), ())), preferred_element_type=jnp.float32
    ).astype(jnp.bfloat16)
    outgoing, tied = lax.optimization_barrier((outgoing, tied))
    latents = lax.all_gather(tied, ("ep", "tp"), axis=0, tiled=True)
    outgoing = outgoing.reshape(ep_size, piece, width)
    arrived = lax.all_to_all(outgoing, "ep", split_axis=0, concat_axis=0, tiled=True)
    summed = group_experts(
        arrived,
        lambda pieces: expert_rows(pieces, local, main, rest, gate_w, up_w, down_w),
    )
    back = lax.all_to_all(summed, "ep", split_axis=0, concat_axis=0, tiled=True).reshape(
        experts * capacity, width
    )
    weights = route_weight / jnp.sum(route_weight, axis=-1, keepdims=True)
    mix = sum(jnp.where(hit, weights[:, k : k + 1], 0.0) for k, hit in enumerate(hits))
    high = mix.astype(jnp.bfloat16)
    low = (mix - high.astype(jnp.float32)).astype(jnp.bfloat16)
    both = jnp.dot(
        jnp.concatenate([high, low], axis=0), back, preferred_element_type=jnp.float32
    )
    return (both[:tok_rows] + both[tok_rows:]).astype(jnp.bfloat16), latents


def plain_device(
    query_latent,
    kv_latent,
    rope_key,
    query_gain,
    kv_gain,
    query_nope_w,
    query_rope_w,
    key_up_w,
    value_up_w,
    output_w,
    expert_in,
    moe_gain,
    routes,
    route_weight,
    gate_w,
    up_w,
    down_w,
):
    front = mixer_front(query_latent, kv_latent, rope_key, query_gain, kv_gain)
    expert_out, latents = experts_half(
        expert_in, moe_gain, routes, route_weight, gate_w, up_w, down_w, front[0]
    )
    mixer_out = mixer(
        (latents,) + front[1:],
        rope_key.shape[1],
        query_nope_w,
        query_rope_w,
        key_up_w,
        value_up_w,
        output_w,
    )
    return (mixer_out, expert_out)


MESH = pl.DeviceIdType.MESH


def partner(index, bits):
    place = 1
    while place <= bits:
        if bits & place:
            index = index + place * (1 - 2 * ((index // place) % 2))
        place *= 2
    return index


class Mail:
    def __init__(self, ep, tp):
        self.ep, self.tp, self.sent = ep, tp, []

    def copy(self, source, target, sems, number, ep=0, tp=0, up=0):
        return pltpu.make_async_remote_copy(
            src_ref=source,
            dst_ref=target,
            send_sem=sems.at[0, number],
            recv_sem=sems.at[1, number],
            device_id=(partner(self.ep, ep) + up, partner(self.tp, tp)),
            device_id_type=MESH,
        )


def expert_step(step, main, rest, recv, lhs, held, gate_w, up_w, down_w):
    local = gate_w.shape[0]
    depth = lhs.shape[1]
    chunks = recv.shape[1] * 2
    mains = chunks * main
    rests = chunks * local * rest
    span = slice(2 * step, 2 * step + 2)
    tail = slice(local * main, local * (main + rest))
    lhs[mains : mains + rests, :] = (
        recv[span, :, tail, :].astype(jnp.float32).reshape(rests, depth).astype(jnp.bfloat16)
    )
    wide = 512

    @pl.loop(0, 1)
    def _(_unused):
        for a in range(local):
            own = slice(a * main, (a + 1) * main)
            lhs[:mains, :] = recv[span, :, own, :].reshape(mains, depth)
            gate = jnp.minimum(
                jnp.dot(lhs[...], gate_w[a], preferred_element_type=jnp.float32), 7.0
            )
            upper = jnp.clip(
                jnp.dot(lhs[...], up_w[a], preferred_element_type=jnp.float32), -7.0, 7.0
            )
            hidden = (gate * jax.nn.sigmoid(1.702 * gate) * (upper + 1.0)).astype(jnp.bfloat16)
            for first in range(0, depth, wide):
                cols = slice(first, first + wide)
                out = jnp.dot(hidden, down_w[a, :, cols], preferred_element_type=jnp.float32)
                recv[span, :, own, cols] = (
                    out[:mains].astype(jnp.bfloat16).reshape(2, chunks // 2, main, wide)
                )
                if a == 0:
                    held[:, cols] = out[mains:]
                else:
                    row = lax.broadcasted_iota(jnp.int32, (rests, wide), 0) % (local * rest)
                    picked = jnp.where(row // rest == a, out[mains:], held[:, cols])
                    if a < local - 1:
                        held[:, cols] = picked
                    else:
                        recv[span, :, tail, cols] = picked.reshape(
                            2, chunks // 2, local * rest, wide
                        ).astype(jnp.bfloat16)


def fused_kernel(
    heads,
    rope,
    main,
    rest,
    outgoing,
    lat_in,
    q_in,
    cos,
    sin,
    query_w,
    key_w,
    value_w,
    output_w,
    gate_h,
    up_h,
    down_h,
    back,
    mixed_out,
    gate_w,
    up_w,
    down_w,
    recv,
    sibling,
    chip,
    far,
    done,
    lhs,
    held,
    lat,
    queries,
    heads_q,
    peak,
    total,
    acc,
    attended,
    mixed,
    mix_sib,
    mix_chip,
    mix_far,
    load_sem,
    go,
    near_a,
    near_b,
    over,
    part,
    ret,
    home,
    lat_sem,
    chain_up,
    chain_sib,
    chain_x,
    chain_xs,
    q_sem,
    mix_sem,
):
    groups = outgoing.shape[0]
    levels = groups // 2
    steps = groups // 2
    rows = lat_in.shape[0]
    ep, tp = lax.axis_index("ep"), lax.axis_index("tp")
    level, y, core = ep // 2, tp // 2, tp % 2
    box = Mail(ep, tp)

    loads = [
        pltpu.make_async_copy(gate_h, gate_w, load_sem.at[0]),
        pltpu.make_async_copy(up_h, up_w, load_sem.at[1]),
        pltpu.make_async_copy(down_h, down_w, load_sem.at[2]),
        pltpu.make_async_copy(outgoing.at[ep], recv.at[0, 0], load_sem.at[3]),
        pltpu.make_async_copy(lat_in, lat.at[ep, y, core], load_sem.at[4]),
        pltpu.make_async_copy(q_in, queries.at[y, core], load_sem.at[5]),
    ]
    for one in loads:
        one.start()

    barrier = pltpu.get_barrier_semaphore()
    for bits in range(1, groups):
        pl.semaphore_signal(
            barrier, inc=1, device_id=(partner(ep, bits), tp), device_id_type=MESH
        )
    for bits in (1, 2):
        pl.semaphore_signal(
            barrier, inc=1, device_id=(ep, partner(tp, bits)), device_id_type=MESH
        )
    pl.semaphore_wait(barrier, groups + 1)

    def dispatch(s):
        return box.copy(outgoing.at[partner(ep, s)], recv.at[s, 0], go, s, ep=s)

    def first(s):
        return outgoing.at[ep] if s == 0 else recv.at[s, 0]

    def to_over(s):
        return box.copy(first(s), recv.at[s, 1], over, s, tp=2)

    def to_near(s):
        return box.copy(first(s), recv.at[s, 2], near_a, s, tp=1)

    def to_near_over(s):
        return box.copy(recv.at[s, 1], recv.at[s, 3], near_b, s, tp=1)

    def to_part(k):
        return box.copy(
            recv.at[2 * k : 2 * k + 2, 2:4], sibling.at[2 * k : 2 * k + 2], part, k, tp=1
        )

    def to_far(s):
        return box.copy(chip.at[s], far.at[s], ret, s, tp=2)

    def to_home(s):
        return box.copy(done.at[s], back.at[ep], home, s, ep=s)

    def forward(s):
        if s:
            dispatch(s).wait_recv()
        to_over(s).start()
        to_near(s).start()

    def cross(s):
        to_over(s).wait_recv()
        to_near_over(s).start()

    def compute(k):
        for s in (2 * k, 2 * k + 1):
            to_near(s).wait_recv()
            to_near_over(s).wait_recv()
            to_over(s).wait_send()
            to_near(s).wait_send()
            to_near_over(s).wait_send()
        expert_step(k, main, rest, recv, lhs, held, gate_w, up_w, down_w)
        to_part(k).start()

    def chip_sum(k):
        to_part(k).wait_recv()
        for s in (2 * k, 2 * k + 1):
            chip[s] = add_rounded(recv[s, 1], sibling[s, 1])
            to_far(s).start()
            recv[s, 0] = add_rounded(recv[s, 0], sibling[s, 0])

    def finish(k):
        for s in (2 * k, 2 * k + 1):
            to_far(s).wait_recv()
            if s == 0:
                back[ep] = add_rounded(recv[s, 0], far[s])
            else:
                done[s] = add_rounded(recv[s, 0], far[s])
                to_home(s).start()

    lat_over = box.copy(lat_in, lat.at[ep, y, core], lat_sem, 0, tp=2)
    lat_near = box.copy(lat_in, lat.at[ep, y, core], lat_sem, 1, tp=1)
    over_block = lat.at[ep, 1 - y, core]
    lat_near_over = box.copy(over_block, over_block, lat_sem, 2, tp=1)
    q_over = box.copy(q_in, queries.at[y, core], q_sem, 0, tp=2)
    q_near = box.copy(q_in, queries.at[y, core], q_sem, 1, tp=1)
    q_over_block = queries.at[1 - y, core]
    q_near_over = box.copy(q_over_block, q_over_block, q_sem, 2, tp=1)

    def blocks(group):
        return lat.at[group, :, core]

    def go_up(k):
        own = blocks(ep - 2 * k)
        return box.copy(own, own, chain_up, k, up=2)

    def go_near(k):
        own = blocks(ep - 2 * k)
        return box.copy(own, own, chain_sib, k, tp=1)

    def go_side(k):
        own = blocks(ep - 2 * k)
        return box.copy(own, own, chain_x, k, ep=1)

    def go_side_near(k):
        own = blocks(partner(ep, 1) - 2 * k)
        return box.copy(own, own, chain_xs, k, tp=1)

    def chain(k):
        @pl.when(level >= k)
        def _():
            if k:
                box.copy(blocks(ep - 2 * k), blocks(ep - 2 * k), chain_up, k - 1, up=2).wait_recv()
                go_near(k).start()
            if k < levels - 1:

                @pl.when(level < levels - 1)
                def _():
                    go_up(k).start()

            go_side(k).start()

    def chain_side(k):
        @pl.when(level >= k)
        def _():
            go_side(k).wait_recv()
            go_side_near(k).start()

    def chain_end(k):
        @pl.when(level >= k)
        def _():
            if k:
                go_near(k).wait_recv()
                go_near(k).wait_send()
            go_side_near(k).wait_recv()
            go_side_near(k).wait_send()
            go_side(k).wait_send()
            if k < levels - 1:

                @pl.when(level < levels - 1)
                def _():
                    go_up(k).wait_send()

    def project_queries():
        flat = jnp.dot(
            queries[...].reshape(4 * rows, queries.shape[3]),
            query_w[...],
            preferred_element_type=jnp.float32,
        )
        nope_all = heads * NOPE
        rope_all = heads * rope
        rot = (
            flat[:, nope_all : nope_all + rope_all] * cos[...]
            + flat[:, nope_all + rope_all :] * sin[...]
        )
        lane = lax.broadcasted_iota(jnp.int32, rot.shape, 1)
        for h in range(heads):
            heads_q[:, h * PAD : h * PAD + NOPE] = flat[:, h * NOPE : (h + 1) * NOPE].astype(
                jnp.bfloat16
            )
            heads_q[:, h * PAD + NOPE : (h + 1) * PAD] = jnp.where(
                lane // rope == h, rot, 0.0
            ).astype(jnp.bfloat16)

    def attention():
        count = 4 * rows
        vdim = value_w.shape[0] // heads
        scale = math.log2(math.e) / math.sqrt(NOPE + rope)
        peak[...] = jnp.full_like(peak, -1e30)
        total[...] = jnp.zeros_like(total)
        acc[...] = jnp.zeros_like(acc)

        def block(number, masked):
            seen = lat[number].reshape(count, lat.shape[4])
            keys = jnp.dot(seen, key_w[...], preferred_element_type=jnp.float32).astype(
                jnp.bfloat16
            )
            vals = lax.dot_general(
                value_w[...], seen, NT, preferred_element_type=jnp.float32
            ).astype(jnp.bfloat16)
            for h in range(heads):
                score = (
                    lax.dot_general(
                        keys[:, h * PAD : (h + 1) * PAD],
                        heads_q[:, h * PAD : (h + 1) * PAD],
                        NT,
                        preferred_element_type=jnp.float32,
                    )
                    * scale
                )
                if masked:
                    key = lax.broadcasted_iota(jnp.int32, score.shape, 0)
                    query = lax.broadcasted_iota(jnp.int32, score.shape, 1)
                    score = jnp.where(key <= query, score, -1e30)
                old = peak[h : h + 1, :]
                new = jnp.maximum(old, jnp.max(score, axis=0, keepdims=True))
                expo = jnp.exp2(score - new)
                factor = jnp.exp2(old - new)
                peak[h : h + 1, :] = new
                total[h : h + 1, :] = total[h : h + 1, :] * factor + jnp.sum(
                    expo, axis=0, keepdims=True
                )
                part_rows = slice(h * vdim, (h + 1) * vdim)
                acc[part_rows, :] = acc[part_rows, :] * factor + jnp.dot(
                    vals[part_rows, :], expo.astype(jnp.bfloat16), preferred_element_type=jnp.float32
                )

        @pl.loop(0, ep)
        def _(number):
            block(number, False)

        block(ep, True)
        for h in range(heads):
            part_rows = slice(h * vdim, (h + 1) * vdim)
            attended[:, part_rows] = (acc[part_rows, :] / total[h : h + 1, :]).T.astype(
                jnp.bfloat16
            )

    def mix(owner_y, owner_core):
        start = pl.multiple_of((owner_y * 2 + owner_core) * rows, rows)
        return jnp.dot(
            attended[pl.ds(start, rows), :], output_w[...], preferred_element_type=jnp.float32
        ).astype(jnp.bfloat16)

    mix_near = box.copy(mixed.at[2:4], mix_sib, mix_sem, 0, tp=1)
    mix_over = box.copy(mix_chip, mix_far, mix_sem, 1, tp=2)

    for s in range(1, groups):
        dispatch(s).start()
    forward(0)
    lat_over.start()
    lat_near.start()
    forward(1)
    cross(0)
    lat_over.wait_recv()
    lat_near_over.start()
    loads[4].wait()
    chain(0)
    q_over.start()
    q_near.start()
    loads[0].wait()
    loads[1].wait()
    loads[2].wait()
    loads[3].wait()
    loads[5].wait()
    for s in (2, 3):
        forward(s)
    cross(1)
    for k in range(steps):
        compute(k)
        for s in (2 * k + 2, 2 * k + 3):
            if s < groups:
                cross(s)
        for s in (2 * k + 4, 2 * k + 5):
            if s < groups:
                forward(s)
        if k == 0:
            q_over.wait_recv()
            q_near_over.start()
            chain_side(0)
        if k:
            chain(k)
        chip_sum(k)
        if k:
            finish(k - 1)
            chain_side(k)
    for k in range(steps, levels):
        chain(k)
        chain_side(k)
    finish(steps - 1)
    q_near.wait_recv()
    q_near_over.wait_recv()
    project_queries()
    lat_near.wait_recv()
    lat_near_over.wait_recv()
    for k in range(levels):
        chain_end(k)
    attention()
    mixed[2] = mix(y, 1 - core)
    mixed[3] = mix(1 - y, 1 - core)
    mix_near.start()
    mixed[0] = mix(y, core)
    mixed[1] = mix(1 - y, core)
    mix_near.wait_recv()
    mix_chip[...] = add_rounded(mixed[1], mix_sib[1])
    mix_over.start()
    mixed[0] = add_rounded(mixed[0], mix_sib[0])
    mix_over.wait_recv()
    mixed_out[...] = add_rounded(mixed[0], mix_far[...])
    for s in range(1, groups):
        to_home(s).wait_recv()
    for s in range(1, groups):
        dispatch(s).wait_send()
        to_home(s).wait_send()
    for s in range(groups):
        to_far(s).wait_send()
    for k in range(steps):
        to_part(k).wait_send()
    for one in (lat_over, lat_near, lat_near_over, q_over, q_near, q_near_over, mix_near, mix_over):
        one.wait_send()


def fused(
    outgoing, lat, query, cos, sin, query_w, key_w, value_w, output_w, gate_w, up_w, down_w, sizes
):
    heads, rope, main, rest = sizes
    groups, piece, depth = outgoing.shape
    rows, lat_width = lat.shape
    local = gate_w.shape[0]
    pair = (2, piece, depth)
    chunks = 8
    mains = chunks * main
    rests = chunks * local * rest
    bf, fl = jnp.bfloat16, jnp.float32
    vmem = pl.BlockSpec(memory_space=pltpu.VMEM)
    hbm = pl.BlockSpec(memory_space=pl.ANY)
    levels = groups // 2
    sem = pltpu.SemaphoreType.DMA
    scratch = [
        pltpu.VMEM(gate_w.shape, bf),
        pltpu.VMEM(up_w.shape, bf),
        pltpu.VMEM(down_w.shape, bf),
        pltpu.VMEM((groups, 4, piece, depth), bf),
        pltpu.VMEM((groups,) + pair, bf),
        pltpu.VMEM((groups, piece, depth), bf),
        pltpu.VMEM((groups, piece, depth), bf),
        pltpu.VMEM((groups, piece, depth), bf),
        pltpu.VMEM((mains + rests, depth), bf),
        pltpu.VMEM((rests, depth), fl),
        pltpu.VMEM((groups, 2, 2, rows, lat_width), bf),
        pltpu.VMEM((2, 2) + query.shape, bf),
        pltpu.VMEM((4 * rows, heads * PAD), bf),
        pltpu.VMEM((heads, 4 * rows), fl),
        pltpu.VMEM((heads, 4 * rows), fl),
        pltpu.VMEM((value_w.shape[0], 4 * rows), fl),
        pltpu.VMEM((4 * rows, value_w.shape[0]), bf),
        pltpu.VMEM((4, rows, depth), bf),
        pltpu.VMEM((2, rows, depth), bf),
        pltpu.VMEM((rows, depth), bf),
        pltpu.VMEM((rows, depth), bf),
        sem((6,)),
        sem((2, groups)),
        sem((2, groups)),
        sem((2, groups)),
        sem((2, groups)),
        sem((2, groups // 2)),
        sem((2, groups)),
        sem((2, groups)),
        sem((2, 3)),
        sem((2, levels)),
        sem((2, levels)),
        sem((2, levels)),
        sem((2, levels)),
        sem((2, 3)),
        sem((2, 2)),
    ]
    return pl.pallas_call(
        functools.partial(fused_kernel, heads, rope, main, rest),
        out_shape=(
            jax.ShapeDtypeStruct(outgoing.shape, bf),
            jax.ShapeDtypeStruct((rows, depth), bf),
        ),
        in_specs=[vmem] * 9 + [hbm] * 3,
        out_specs=(vmem, vmem),
        scratch_shapes=scratch,
        compiler_params=pltpu.CompilerParams(
            collective_id=0, has_side_effects=True, vmem_limit_bytes=60 * 1024 * 1024
        ),
    )(outgoing, lat, query, cos, sin, query_w, key_w, value_w, output_w, gate_w, up_w, down_w)


def per_device(
    query_latent,
    kv_latent,
    rope_key,
    query_gain,
    kv_gain,
    query_nope_w,
    query_rope_w,
    key_up_w,
    value_up_w,
    output_w,
    expert_in,
    moe_gain,
    routes,
    route_weight,
    gate_w,
    up_w,
    down_w,
):
    tok_rows, top_count = routes.shape
    width = expert_in.shape[1]
    local = gate_w.shape[0]
    rope = rope_key.shape[1]
    heads = query_nope_w.shape[1] // NOPE
    ep_size, tp_size = lax.axis_size("ep"), lax.axis_size("tp")
    experts = local * ep_size
    capacity = max(2, 5 * tok_rows * top_count // (4 * experts))
    main = capacity // 8 * 8
    rest = capacity - main
    if not (
        tp_size == 4
        and ep_size & (ep_size - 1) == 0
        and main % 16 == 0
        and local * rest % 8 == 0
        and heads * rope == 128
    ):
        return plain_device(
            query_latent,
            kv_latent,
            rope_key,
            query_gain,
            kv_gain,
            query_nope_w,
            query_rope_w,
            key_up_w,
            value_up_w,
            output_w,
            expert_in,
            moe_gain,
            routes,
            route_weight,
            gate_w,
            up_w,
            down_w,
        )
    half = rope // 2
    group_rows = tok_rows * tp_size
    freq = 1.0 / THETA ** (jnp.arange(half, dtype=jnp.float32) * 2.0 / rope)
    first_pos = lax.axis_index("ep") * group_rows
    positions = first_pos + jnp.arange(group_rows, dtype=jnp.int32)
    own = lax.axis_index("tp") * tok_rows + first_pos + jnp.arange(tok_rows, dtype=jnp.int32)
    own_angle = own.astype(jnp.float32)[:, None] * jnp.tile(freq, 2)[None, :]
    keys = rope_key.astype(jnp.float32)
    turned = jnp.concatenate([-keys[:, half:], keys[:, :half]], axis=-1)
    key_rot = (keys * jnp.cos(own_angle) + turned * jnp.sin(own_angle)).astype(jnp.bfloat16)
    own_latents = jnp.concatenate([rms_scale(kv_latent, kv_gain), key_rot], axis=1)
    own_query = rms_scale(query_latent, query_gain)
    angle = positions.astype(jnp.float32)[:, None] * jnp.tile(freq, 2 * heads)[None, :]
    turned_w = []
    for h in range(heads):
        turned_w.append(-query_rope_w[:, h * rope + half : (h + 1) * rope])
        turned_w.append(query_rope_w[:, h * rope : h * rope + half])
    query_w = jnp.concatenate([query_nope_w, query_rope_w] + turned_w, axis=1)
    key_w = jnp.concatenate(
        [
            jnp.concatenate(
                [
                    jnp.pad(key_up_w[:, h * NOPE : (h + 1) * NOPE], ((0, 0), (0, PAD - NOPE))),
                    jnp.pad(
                        jnp.eye(rope, dtype=jnp.bfloat16),
                        ((0, 0), (NOPE + h * rope, PAD - NOPE - (h + 1) * rope)),
                    ),
                ],
                axis=0,
            )
            for h in range(heads)
        ],
        axis=1,
    )
    value_w = jnp.pad(value_up_w.T, ((0, 0), (0, rope)))
    floats = expert_in.astype(jnp.float32)
    center = floats - jnp.mean(floats, axis=-1, keepdims=True)
    variance = jnp.mean(center * center, axis=-1, keepdims=True)
    normed_in = (center * lax.rsqrt(variance + 1e-05) * moe_gain).astype(jnp.bfloat16)
    hits = route(routes, experts, local, capacity)
    select = functools.reduce(jnp.logical_or, hits).astype(jnp.bfloat16)
    outgoing = (
        lax.dot_general(select, normed_in, (((0,), (0,)), ((), ())), preferred_element_type=jnp.float32)
        .astype(jnp.bfloat16)
        .reshape(ep_size, local * capacity, width)
    )
    back, mixer_out = fused(
        outgoing,
        own_latents,
        own_query,
        jnp.cos(angle),
        jnp.sin(angle),
        query_w,
        key_w,
        value_w,
        output_w,
        gate_w,
        up_w,
        down_w,
        (heads, rope, main, rest),
    )
    back = back.reshape(experts * capacity, width)
    weights = route_weight / jnp.sum(route_weight, axis=-1, keepdims=True)
    mix = sum(jnp.where(hit, weights[:, k : k + 1], 0.0) for k, hit in enumerate(hits))
    high = mix.astype(jnp.bfloat16)
    low = (mix - high.astype(jnp.float32)).astype(jnp.bfloat16)
    both = jnp.dot(jnp.concatenate([high, low], axis=0), back, preferred_element_type=jnp.float32)
    return mixer_out, (both[:tok_rows] + both[tok_rows:]).astype(jnp.bfloat16)


def solution(mesh):
    placed = (
        P(("ep", "tp"), None),
        P(("ep", "tp"), None),
        P(("ep", "tp"), None),
        P(),
        P(),
        P(None, "tp"),
        P(None, "tp"),
        P(None, "tp"),
        P(None, "tp"),
        P("tp", None),
        P(("ep", "tp"), None),
        P(),
        P(("ep", "tp"), None),
        P(("ep", "tp"), None),
        P("ep", None, "tp"),
        P("ep", None, "tp"),
        P("ep", "tp", None),
    )
    return jax.shard_map(
        per_device,
        mesh=mesh,
        in_specs=placed,
        out_specs=(P(("ep", "tp"), None), P(("ep", "tp"), None)),
        check_vma=False,
    )
```

```python
import functools
import math

import jax
import jax.numpy as jnp
import numpy as np
from jax import lax
from jax.experimental import pallas as pl
from jax.experimental.pallas import tpu as pltpu
from jax.sharding import PartitionSpec as P

NOPE = 128


THETA = 10000.0

PAD = 256

NT = (((1,), (1,)), ((), ()))


def rms_scale(values, gain):
    floats = values.astype(jnp.float32)
    square = jnp.mean(floats * floats, axis=-1, keepdims=True)
    return (floats * lax.rsqrt(square + 1e-06) * gain).astype(jnp.bfloat16)


def attend_kernel(heads, rope, last_ref, lat_ref, q_ref, wk_ref, wv_ref, out_ref, peak, total, acc):
    rows = q_ref.shape[0]
    vdim = wv_ref.shape[0] // heads
    scale = math.log2(math.e) / math.sqrt(NOPE + rope)
    peak[...] = jnp.full_like(peak, -1e30)
    total[...] = jnp.zeros_like(total)
    acc[...] = jnp.zeros_like(acc)

    def block(number, masked):
        lat = lat_ref[pl.ds(pl.multiple_of(number * rows, rows), rows), :]
        keys = jnp.dot(lat, wk_ref[...], preferred_element_type=jnp.float32).astype(jnp.bfloat16)
        vals = lax.dot_general(
            wv_ref[...], lat, NT, preferred_element_type=jnp.float32
        ).astype(jnp.bfloat16)
        for h in range(heads):
            score = (
                lax.dot_general(
                    keys[:, h * PAD : (h + 1) * PAD],
                    q_ref[:, h * PAD : (h + 1) * PAD],
                    NT,
                    preferred_element_type=jnp.float32,
                )
                * scale
            )
            if masked:
                key = lax.broadcasted_iota(jnp.int32, score.shape, 0)
                query = lax.broadcasted_iota(jnp.int32, score.shape, 1)
                score = jnp.where(key <= query, score, -1e30)
            old = peak[h : h + 1, :]
            new = jnp.maximum(old, jnp.max(score, axis=0, keepdims=True))
            expo = jnp.exp2(score - new)
            factor = jnp.exp2(old - new)
            peak[h : h + 1, :] = new
            total[h : h + 1, :] = total[h : h + 1, :] * factor + jnp.sum(
                expo, axis=0, keepdims=True
            )
            part = slice(h * vdim, (h + 1) * vdim)
            acc[part, :] = acc[part, :] * factor + jnp.dot(
                vals[part, :], expo.astype(jnp.bfloat16), preferred_element_type=jnp.float32
            )

    last = last_ref[0]

    @pl.loop(0, last)
    def _(number):
        block(number, False)

    block(last, True)
    for h in range(heads):
        part = slice(h * vdim, (h + 1) * vdim)
        out_ref[part, :] = (acc[part, :] / total[h : h + 1, :]).astype(jnp.bfloat16)


def attend(last, latents, queries, key_w, value_w, heads, rope):
    rows = queries.shape[0]
    vdim_all = value_w.shape[0]
    vmem = pl.BlockSpec(memory_space=pltpu.VMEM)
    length = latents.shape[0]
    return pl.pallas_call(
        functools.partial(attend_kernel, heads, rope),
        out_shape=jax.ShapeDtypeStruct((vdim_all, rows), jnp.bfloat16),
        in_specs=[pl.BlockSpec(memory_space=pltpu.SMEM)] + [vmem] * 4,
        out_specs=vmem,
        scratch_shapes=[
            pltpu.VMEM((heads, rows), jnp.float32),
            pltpu.VMEM((heads, rows), jnp.float32),
            pltpu.VMEM((vdim_all, rows), jnp.float32),
        ],
        compiler_params=pltpu.CompilerParams(vmem_limit_bytes=40 * 1024 * 1024),
        cost_estimate=pl.CostEstimate(
            flops=2 * length * rows * heads * (PAD + 2 * NOPE),
            bytes_accessed=latents.size * 2,
            transcendentals=length * rows * heads,
        ),
    )(last, latents, queries, key_w, value_w)


def mixer_front(query_latent, kv_latent, rope_key, query_gain, kv_gain):
    tok_rows = query_latent.shape[0]
    rope = rope_key.shape[1]
    half = rope // 2
    group_rows = tok_rows * lax.axis_size("tp")
    freq = 1.0 / THETA ** (jnp.arange(half, dtype=jnp.float32) * 2.0 / rope)
    first_pos = lax.axis_index("ep") * group_rows
    positions = first_pos + jnp.arange(group_rows, dtype=jnp.int32)
    own = lax.axis_index("tp") * tok_rows + first_pos + jnp.arange(tok_rows, dtype=jnp.int32)
    angle = own.astype(jnp.float32)[:, None] * jnp.tile(freq, 2)[None, :]
    keys = rope_key.astype(jnp.float32)
    turned = jnp.concatenate([-keys[:, half:], keys[:, :half]], axis=-1)
    key_rot = (keys * jnp.cos(angle) + turned * jnp.sin(angle)).astype(jnp.bfloat16)
    kv_normed = rms_scale(kv_latent, kv_gain)
    own_latents = jnp.concatenate([kv_normed, key_rot], axis=1)
    query_normed = lax.all_gather(rms_scale(query_latent, query_gain), "tp", axis=0, tiled=True)
    return own_latents, query_normed, positions, freq


def mixer(
    front, rope, query_nope_w, query_rope_w, key_up_w, value_up_w, output_w
):
    latents, query_normed, positions, freq = front
    half = rope // 2
    heads = query_nope_w.shape[1] // NOPE
    kv_width = key_up_w.shape[0]
    angle = positions.astype(jnp.float32)[:, None] * jnp.tile(freq, 2 * heads)[None, :]
    turned_w = []
    for h in range(heads):
        turned_w.append(-query_rope_w[:, h * rope + half : (h + 1) * rope])
        turned_w.append(query_rope_w[:, h * rope : h * rope + half])
    weights = jnp.concatenate([query_nope_w, query_rope_w] + turned_w, axis=1)
    flat = jnp.dot(query_normed, weights, preferred_element_type=jnp.float32)
    nope_all = heads * NOPE
    rope_all = heads * rope
    rot = (
        flat[:, nope_all : nope_all + rope_all] * jnp.cos(angle)
        + flat[:, nope_all + rope_all :] * jnp.sin(angle)
    ).astype(jnp.bfloat16)
    query_flat = flat[:, :nope_all].astype(jnp.bfloat16)
    blank = jnp.zeros((flat.shape[0], PAD - NOPE - rope), jnp.bfloat16)
    pieces = []
    for h in range(heads):
        pieces += [
            query_flat[:, h * NOPE : (h + 1) * NOPE],
            rot[:, h * rope : (h + 1) * rope],
            blank,
        ]
    queries = jnp.concatenate(pieces, axis=1)
    carry = jnp.pad(
        jnp.eye(rope, dtype=jnp.bfloat16), ((0, 0), (NOPE, PAD - NOPE - rope))
    )
    key_w = jnp.concatenate(
        [
            jnp.concatenate(
                [
                    jnp.pad(key_up_w[:, h * NOPE : (h + 1) * NOPE], ((0, 0), (0, PAD - NOPE))),
                    carry,
                ],
                axis=0,
            )
            for h in range(heads)
        ],
        axis=1,
    )
    value_w = jnp.pad(value_up_w.T, ((0, 0), (0, latents.shape[1] - kv_width)))
    last = lax.axis_index("ep").astype(jnp.int32).reshape(1)
    attended = attend(last, latents, queries, key_w, value_w, heads, rope)
    mixed = lax.dot_general(
        attended, output_w, (((0,), (0,)), ((), ())), preferred_element_type=jnp.float32
    ).astype(jnp.bfloat16)
    return lax.psum_scatter(mixed, "tp", scatter_dimension=0, tiled=True)


def route(routes, experts, local, capacity):
    rows = routes.shape[0]
    main = capacity // 8 * 8
    rest = capacity - main
    names = jnp.arange(experts, dtype=jnp.int32)[None, :]
    chosen = [routes[:, k : k + 1] == names for k in range(routes.shape[1])]
    member = functools.reduce(jnp.logical_or, chosen).astype(jnp.bfloat16)
    before = lax.broadcasted_iota(jnp.int32, (rows, rows), 0) > lax.broadcasted_iota(
        jnp.int32, (rows, rows), 1
    )
    rank = jnp.dot(
        before.astype(jnp.bfloat16), member, preferred_element_type=jnp.float32
    ).astype(jnp.int32)
    inner = names % local
    place = jnp.where(
        rank < main, inner * main + rank, local * main + inner * rest + rank - main
    ) + names // local * (local * capacity)
    slots = lax.broadcasted_iota(jnp.int32, (rows, experts * capacity), 1)
    return [
        jnp.sum(jnp.where(one, place, 0), axis=1, keepdims=True) == slots for one in chosen
    ]


def swap(values, bit):
    size = lax.axis_size("tp")
    return lax.ppermute(values, "tp", [(one, one ^ bit) for one in range(size)])


def expert_rows(pieces, local, main, rest, gate_w, up_w, down_w):
    groups, piece, width = pieces.shape
    mixed = pieces[:, local * main :].reshape(groups * local * rest, width)
    owner = (
        lax.broadcasted_iota(jnp.int32, (groups * local * rest, 1), 0) % (local * rest)
    ) // max(rest, 1)
    mains = []
    shared = 0.0
    for expert in range(local):
        inputs = jnp.concatenate(
            [
                pieces[:, expert * main : (expert + 1) * main].reshape(groups * main, width),
                mixed,
            ],
            axis=0,
        )
        gate = jnp.minimum(jnp.dot(inputs, gate_w[expert], preferred_element_type=jnp.float32), 7.0)
        upper = jnp.clip(
            jnp.dot(inputs, up_w[expert], preferred_element_type=jnp.float32), -7.0, 7.0
        )
        hidden = (gate * jax.nn.sigmoid(1.702 * gate) * (upper + 1.0)).astype(jnp.bfloat16)
        output = jnp.dot(hidden, down_w[expert], preferred_element_type=jnp.float32).astype(
            jnp.bfloat16
        )
        mains.append(output[: groups * main].reshape(groups, main, width))
        shared = jnp.where(owner == expert, output[groups * main :], shared)
    shared = shared.astype(jnp.bfloat16).reshape(groups, local * rest, width)
    return jnp.concatenate(mains + [shared], axis=1)


def add_rounded(one, other):
    return (one.astype(jnp.float32) + other.astype(jnp.float32)).astype(jnp.bfloat16)


def group_experts(arrived, run):
    size = lax.axis_size("tp")
    if size & (size - 1):
        spread = lax.all_gather(arrived, "tp", axis=0, tiled=True)
        return lax.psum_scatter(run(spread), "tp", scatter_dimension=0, tiled=True)
    count = arrived.shape[0]
    far = {0: arrived}
    for bit in [1 << k for k in range(1, size.bit_length() - 1)]:
        for key in sorted(far):
            far[key | bit] = swap(far[key], bit)
    results = {}
    for key in sorted(far):
        if size == 1:
            results[key] = run(far[key])
            continue
        near = swap(far[key], 1)
        both = run(jnp.concatenate([far[key], near], axis=0))
        results[key] = add_rounded(both[:count], swap(both[count:], 1))
    for bit in [1 << k for k in range(size.bit_length() - 2, 0, -1)]:
        for key in sorted(results):
            if key & bit:
                results[key ^ bit] = add_rounded(results[key ^ bit], swap(results.pop(key), bit))
    return results[0]


def experts_half(expert_in, moe_gain, routes, route_weight, gate_w, up_w, down_w, tied):
    tok_rows, top_count = routes.shape
    width = expert_in.shape[1]
    local = gate_w.shape[0]
    ep_size = lax.axis_size("ep")
    experts = local * ep_size
    capacity = max(2, 5 * tok_rows * top_count // (4 * experts))
    main = capacity // 8 * 8
    rest = capacity - main
    piece = local * capacity
    floats = expert_in.astype(jnp.float32)
    center = floats - jnp.mean(floats, axis=-1, keepdims=True)
    variance = jnp.mean(center * center, axis=-1, keepdims=True)
    normed_in = (center * lax.rsqrt(variance + 1e-05) * moe_gain).astype(jnp.bfloat16)
    hits = route(routes, experts, local, capacity)
    select = functools.reduce(jnp.logical_or, hits).astype(jnp.bfloat16)
    outgoing = lax.dot_general(
        select, normed_in, (((0,), (0,)), ((), ())), preferred_element_type=jnp.float32
    ).astype(jnp.bfloat16)
    outgoing, tied = lax.optimization_barrier((outgoing, tied))
    latents = lax.all_gather(tied, ("ep", "tp"), axis=0, tiled=True)
    outgoing = outgoing.reshape(ep_size, piece, width)
    arrived = lax.all_to_all(outgoing, "ep", split_axis=0, concat_axis=0, tiled=True)
    summed = group_experts(
        arrived,
        lambda pieces: expert_rows(pieces, local, main, rest, gate_w, up_w, down_w),
    )
    back = lax.all_to_all(summed, "ep", split_axis=0, concat_axis=0, tiled=True).reshape(
        experts * capacity, width
    )
    weights = route_weight / jnp.sum(route_weight, axis=-1, keepdims=True)
    mix = sum(jnp.where(hit, weights[:, k : k + 1], 0.0) for k, hit in enumerate(hits))
    high = mix.astype(jnp.bfloat16)
    low = (mix - high.astype(jnp.float32)).astype(jnp.bfloat16)
    both = jnp.dot(
        jnp.concatenate([high, low], axis=0), back, preferred_element_type=jnp.float32
    )
    return (both[:tok_rows] + both[tok_rows:]).astype(jnp.bfloat16), latents


def plain_device(
    query_latent,
    kv_latent,
    rope_key,
    query_gain,
    kv_gain,
    query_nope_w,
    query_rope_w,
    key_up_w,
    value_up_w,
    output_w,
    expert_in,
    moe_gain,
    routes,
    route_weight,
    gate_w,
    up_w,
    down_w,
):
    front = mixer_front(query_latent, kv_latent, rope_key, query_gain, kv_gain)
    expert_out, latents = experts_half(
        expert_in, moe_gain, routes, route_weight, gate_w, up_w, down_w, front[0]
    )
    mixer_out = mixer(
        (latents,) + front[1:],
        rope_key.shape[1],
        query_nope_w,
        query_rope_w,
        key_up_w,
        value_up_w,
        output_w,
    )
    return (mixer_out, expert_out)


MESH = pl.DeviceIdType.MESH


def partner(index, bits):
    place = 1
    while place <= bits:
        if bits & place:
            index = index + place * (1 - 2 * ((index // place) % 2))
        place *= 2
    return index


def scoped(name):
    def wrap(inner):
        def run(*args):
            with jax.named_scope(name + "".join(str(a) for a in args if isinstance(a, int))):
                return inner(*args)

        return run

    return wrap


class Mail:
    def __init__(self, ep, tp):
        self.ep, self.tp, self.sent = ep, tp, []

    def copy(self, source, target, sems, number, ep=0, tp=0, up=0):
        return pltpu.make_async_remote_copy(
            src_ref=source,
            dst_ref=target,
            send_sem=sems.at[0, number],
            recv_sem=sems.at[1, number],
            device_id=(partner(self.ep, ep) + up, partner(self.tp, tp)),
            device_id_type=MESH,
        )


def expert_step(step, main, rest, recv, lhs, held, gate_w, up_w, down_w):
    local = gate_w.shape[0]
    depth = lhs.shape[1]
    chunks = recv.shape[1] * 2
    mains = chunks * main
    rests = chunks * local * rest
    span = slice(2 * step, 2 * step + 2)
    tail = slice(local * main, local * (main + rest))
    lhs[mains : mains + rests, :] = (
        recv[span, :, tail, :].astype(jnp.float32).reshape(rests, depth).astype(jnp.bfloat16)
    )
    wide = 512

    if True:
        for a in range(local):
            own = slice(a * main, (a + 1) * main)
            lhs[:mains, :] = recv[span, :, own, :].reshape(mains, depth)
            gate = jnp.minimum(
                jnp.dot(lhs[...], gate_w[a], preferred_element_type=jnp.float32), 7.0
            )
            upper = jnp.clip(
                jnp.dot(lhs[...], up_w[a], preferred_element_type=jnp.float32), -7.0, 7.0
            )
            hidden = (gate * jax.nn.sigmoid(1.702 * gate) * (upper + 1.0)).astype(jnp.bfloat16)
            for first in range(0, depth, wide):
                cols = slice(first, first + wide)
                out = jnp.dot(hidden, down_w[a, :, cols], preferred_element_type=jnp.float32)
                recv[span, :, own, cols] = (
                    out[:mains].astype(jnp.bfloat16).reshape(2, chunks // 2, main, wide)
                )
                if a == 0:
                    held[:, cols] = out[mains:]
                else:
                    row = lax.broadcasted_iota(jnp.int32, (rests, wide), 0) % (local * rest)
                    picked = jnp.where(row // rest == a, out[mains:], held[:, cols])
                    if a < local - 1:
                        held[:, cols] = picked
                    else:
                        recv[span, :, tail, cols] = picked.reshape(
                            2, chunks // 2, local * rest, wide
                        ).astype(jnp.bfloat16)


def prepare_rows(local, main, rest, rows_in, moe_gain, routes, route_weight, outgoing, shares):
    groups, piece, depth = outgoing.shape
    rows = rows_in.shape[0]
    experts = groups * local
    floats = rows_in[...].astype(jnp.float32)
    center = floats - jnp.mean(floats, axis=-1, keepdims=True)
    variance = jnp.mean(center * center, axis=-1, keepdims=True)
    normed = (center * lax.rsqrt(variance + 1e-05) * moe_gain[...][None, :]).astype(jnp.bfloat16)
    chosen = [routes[k : k + 1, :] for k in range(routes.shape[0])]
    names = lax.broadcasted_iota(jnp.int32, (experts, rows), 0)
    match = [one == names for one in chosen]
    member = jnp.where(functools.reduce(jnp.logical_or, match), 1.0, 0.0).astype(jnp.bfloat16)
    before = lax.broadcasted_iota(jnp.int32, (rows, rows), 0) < lax.broadcasted_iota(
        jnp.int32, (rows, rows), 1
    )
    rank = jnp.dot(
        member, jnp.where(before, 1.0, 0.0).astype(jnp.bfloat16), preferred_element_type=jnp.float32
    )
    inner = (names % local).astype(jnp.float32)
    start = ((names // local) * piece).astype(jnp.float32)
    place = start + jnp.where(
        rank < main, inner * main + rank, local * main + inner * rest + rank - main
    )
    places = [
        jnp.sum(jnp.where(one, place, 0.0), axis=0, keepdims=True).astype(jnp.int32)
        for one in match
    ]
    slots = lax.broadcasted_iota(jnp.int32, (groups * piece, rows), 0)
    hits = [one == slots for one in places]
    select = jnp.where(functools.reduce(jnp.logical_or, hits), 1.0, 0.0).astype(jnp.bfloat16)
    outgoing[...] = (
        jnp.dot(select, normed, preferred_element_type=jnp.float32)
        .reshape(groups, piece, depth)
        .astype(jnp.bfloat16)
    )
    loads = [route_weight[k : k + 1, :] for k in range(routes.shape[0])]
    whole = sum(loads)
    share = sum(jnp.where(hit, one / whole, 0.0) for hit, one in zip(hits, loads))
    high = share.astype(jnp.bfloat16).astype(jnp.float32)
    shares[:, :, :rows] = high.reshape(groups, piece, rows).astype(jnp.bfloat16)
    shares[:, :, rows:] = (share - high).reshape(groups, piece, rows).astype(jnp.bfloat16)


def fused_kernel(
    heads,
    rope,
    main,
    rest,
    query_in,
    kv_in,
    rope_in,
    query_gain,
    kv_gain,
    freq,
    moe_gain,
    routes,
    route_weight,
    rows_h,
    nope_h,
    rope_h,
    key_h,
    value_h,
    output_h,
    gate_h,
    up_h,
    down_h,
    mixed_out,
    expert_out,
    rows_in,
    outgoing,
    back,
    shares,
    blend,
    nope_w,
    rope_w,
    key_w,
    value_w,
    output_w,
    value_t,
    keys_s,
    gate_w,
    up_w,
    down_w,
    recv,
    sibling,
    chip,
    far,
    done,
    lhs,
    held,
    lat,
    wide_key,
    queries,
    heads_q,
    peak,
    total,
    acc,
    attended,
    mixed,
    mix_sib,
    mix_chip,
    mix_far,
    load_sem,
    go,
    near_a,
    near_b,
    over,
    part,
    ret,
    home,
    lat_sem,
    chain_up,
    chain_sib,
    chain_x,
    chain_xs,
    q_sem,
    mix_sem,
):
    groups = outgoing.shape[0]
    local = gate_w.shape[0]
    levels = groups // 2
    steps = groups // 2
    rows = kv_in.shape[0]
    kv_width = kv_in.shape[1]
    ep, tp = lax.axis_index("ep"), lax.axis_index("tp")
    half = rope // 2
    level, y, core = ep // 2, tp // 2, tp % 2
    box = Mail(ep, tp)

    loads = [
        pltpu.make_async_copy(gate_h, gate_w, load_sem.at[0]),
        pltpu.make_async_copy(up_h, up_w, load_sem.at[1]),
        pltpu.make_async_copy(down_h, down_w, load_sem.at[2]),
        pltpu.make_async_copy(rows_h, rows_in, load_sem.at[3]),
        pltpu.make_async_copy(nope_h, nope_w, load_sem.at[4]),
        pltpu.make_async_copy(rope_h, rope_w, load_sem.at[5]),
        pltpu.make_async_copy(key_h, key_w, load_sem.at[6]),
        pltpu.make_async_copy(value_h, value_w, load_sem.at[7]),
        pltpu.make_async_copy(output_h, output_w, load_sem.at[8]),
    ]
    for one in loads[3:] + loads[:3]:
        one.start()

    barrier = pltpu.get_barrier_semaphore()
    for bits in range(1, groups):
        pl.semaphore_signal(
            barrier, inc=1, device_id=(partner(ep, bits), tp), device_id_type=MESH
        )
    for bits in (1, 2):
        pl.semaphore_signal(
            barrier, inc=1, device_id=(ep, partner(tp, bits)), device_id_type=MESH
        )
    lane = lax.broadcasted_iota(jnp.int32, (rows, 128), 1)
    place = lax.broadcasted_iota(jnp.int32, (rows, 128), 0) + lane // half * rows
    angle = (place + ep * (4 * rows)).astype(jnp.float32) * freq[...]
    cos_all, sin_all = jnp.cos(angle), jnp.sin(angle)

    def spread(table, block):
        own = jnp.where(lane // half == block, table, 0.0)
        own = own + pltpu.roll(own, half, 1)
        return own + pltpu.roll(own, 2 * half, 1)

    def rotate(values, block):
        turned = jnp.where(
            lane % rope < half, -pltpu.roll(values, 128 - half, 1), pltpu.roll(values, half, 1)
        )
        return values * spread(cos_all, block) + turned * spread(sin_all, block)

    scope = jax.named_scope("latents")
    scope.__enter__()
    lat[ep, y, core, :, :kv_width] = rms_scale(kv_in[...], kv_gain[...][None, :])
    raw_key = rope_in[...].astype(jnp.float32).T
    wide_key[:, :rope] = raw_key
    wide_key[:, rope:] = raw_key
    lat[ep, y, core, :, kv_width:] = rotate(wide_key[...], tp)[:, :rope].astype(jnp.bfloat16)
    queries[y, core] = rms_scale(query_in[...], query_gain[...][None, :])
    scope.__exit__(None, None, None)
    with jax.named_scope("barrier"):
        pl.semaphore_wait(barrier, groups + 1)

    def dispatch(s):
        return box.copy(outgoing.at[partner(ep, s)], recv.at[s, 0], go, s, ep=s)

    def first(s):
        return outgoing.at[ep] if s == 0 else recv.at[s, 0]

    def to_over(s):
        return box.copy(first(s), recv.at[s, 1], over, s, tp=2)

    def to_near(s):
        return box.copy(first(s), recv.at[s, 2], near_a, s, tp=1)

    def to_near_over(s):
        return box.copy(recv.at[s, 1], recv.at[s, 3], near_b, s, tp=1)

    def to_part(k):
        return box.copy(
            recv.at[2 * k : 2 * k + 2, 2:4], sibling.at[2 * k : 2 * k + 2], part, k, tp=1
        )

    def to_far(s):
        return box.copy(chip.at[s], far.at[s], ret, s, tp=2)

    def to_home(s):
        return box.copy(done.at[s], back.at[ep], home, s, ep=s)

    @scoped("forward")
    def forward(s):
        if s:
            dispatch(s).wait_recv()
        to_over(s).start()
        to_near(s).start()

    @scoped("cross")
    def cross(s):
        to_over(s).wait_recv()
        to_near_over(s).start()

    @scoped("compute")
    def compute(k):
        for s in (2 * k, 2 * k + 1):
            to_near(s).wait_recv()
            to_near_over(s).wait_recv()
            to_over(s).wait_send()
            to_near(s).wait_send()
            to_near_over(s).wait_send()
        with jax.named_scope(f"expert{k}"):
            expert_step(k, main, rest, recv, lhs, held, gate_w, up_w, down_w)
        to_part(k).start()

    @scoped("chip_sum")
    def chip_sum(k):
        to_part(k).wait_recv()
        for s in (2 * k, 2 * k + 1):
            chip[s] = add_rounded(recv[s, 1], sibling[s, 1])
            if k >= groups // 4:
                to_far(s).start()
            recv[s, 0] = add_rounded(recv[s, 0], sibling[s, 0])

    @scoped("finish")
    def finish(k):
        for s in (2 * k, 2 * k + 1):
            to_far(s).wait_recv()
            if s == 0:
                back[ep] = add_rounded(recv[s, 0], far[s])
            else:
                done[s] = add_rounded(recv[s, 0], far[s])
                to_home(s).start()

    own_block, own_query = lat.at[ep, y, core], queries.at[y, core]
    lat_over = box.copy(own_block, own_block, lat_sem, 0, tp=2)
    lat_near = box.copy(own_block, own_block, lat_sem, 1, tp=1)
    over_block = lat.at[ep, 1 - y, core]
    lat_near_over = box.copy(over_block, over_block, lat_sem, 2, tp=1)
    q_over = box.copy(own_query, own_query, q_sem, 0, tp=2)
    q_near = box.copy(own_query, own_query, q_sem, 1, tp=1)
    q_over_block = queries.at[1 - y, core]
    q_near_over = box.copy(q_over_block, q_over_block, q_sem, 2, tp=1)

    def blocks(group):
        return lat.at[group, :, core]

    def go_up(k):
        own = blocks(ep - 2 * k)
        return box.copy(own, own, chain_up, k, up=2)

    def go_near(k):
        own = blocks(ep - 2 * k)
        return box.copy(own, own, chain_sib, k, tp=1)

    def go_side(k):
        own = blocks(ep - 2 * k)
        return box.copy(own, own, chain_x, k, ep=1)

    def go_side_near(k):
        own = blocks(partner(ep, 1) - 2 * k)
        return box.copy(own, own, chain_xs, k, tp=1)

    @scoped("chain")
    def chain(k):
        @pl.when(level >= k)
        def _():
            if k:
                box.copy(blocks(ep - 2 * k), blocks(ep - 2 * k), chain_up, k - 1, up=2).wait_recv()
                go_near(k).start()
            if k < levels - 1:

                @pl.when(level < levels - 1)
                def _():
                    go_up(k).start()

            go_side(k).start()

    @scoped("chain_side")
    def chain_side(k):
        @pl.when(level >= k)
        def _():
            go_side(k).wait_recv()
            go_side_near(k).start()

    @scoped("chain_end")
    def chain_end(k):
        @pl.when(level >= k)
        def _():
            if k:
                go_near(k).wait_recv()
                go_near(k).wait_send()
            go_side_near(k).wait_recv()
            go_side_near(k).wait_send()
            go_side(k).wait_send()
            if k < levels - 1:

                @pl.when(level < levels - 1)
                def _():
                    go_up(k).wait_send()

    @scoped("project_queries")
    def project_queries():
        for block in range(4):
            source = queries[block // 2, block % 2]
            span = slice(block * rows, (block + 1) * rows)
            flat = jnp.dot(source, nope_w[...], preferred_element_type=jnp.float32)
            rot = rotate(
                jnp.dot(source, rope_w[...], preferred_element_type=jnp.float32), block
            )
            for h in range(heads):
                heads_q[span, h * PAD : h * PAD + NOPE] = flat[
                    :, h * NOPE : (h + 1) * NOPE
                ].astype(jnp.bfloat16)
                shifted = pltpu.roll(rot, 128 - h * rope, 1) if h else rot
                heads_q[span, h * PAD + NOPE : (h + 1) * PAD] = jnp.where(
                    lane < rope, shifted, 0.0
                ).astype(jnp.bfloat16)

    count = 4 * rows
    vdim = value_w.shape[1] // heads
    scale = math.log2(math.e) / math.sqrt(NOPE + rope)

    @scoped("attend_start")
    def attend_start():
        peak[...] = jnp.full_like(peak, -1e30)
        total[...] = jnp.zeros_like(total)
        acc[...] = jnp.zeros_like(acc)
        value_t[...] = value_w[...].astype(jnp.float32).T.astype(jnp.bfloat16)
        for h in range(heads):
            keys_s[:, h * PAD + NOPE : (h + 1) * PAD] = jnp.zeros(
                (count, PAD - NOPE), jnp.bfloat16
            )

    def attend_block(number, masked):
        seen = lat[number, :, :, :, :kv_width].reshape(count, kv_width)
        turned_key = lat[number, :, :, :, kv_width:].reshape(count, rope)
        flat = jnp.dot(seen, key_w[...], preferred_element_type=jnp.float32)
        vals = lax.dot_general(
            value_t[...], seen, NT, preferred_element_type=jnp.float32
        ).astype(jnp.bfloat16)
        for h in range(heads):
            keys_s[:, h * PAD : h * PAD + NOPE] = flat[:, h * NOPE : (h + 1) * NOPE].astype(
                jnp.bfloat16
            )
            keys_s[:, h * PAD + NOPE : h * PAD + NOPE + rope] = turned_key
        for h in range(heads):
            score = (
                lax.dot_general(
                    keys_s[:, h * PAD : (h + 1) * PAD],
                    heads_q[:, h * PAD : (h + 1) * PAD],
                    NT,
                    preferred_element_type=jnp.float32,
                )
                * scale
            )
            if masked:
                key = lax.broadcasted_iota(jnp.int32, score.shape, 0)
                query = lax.broadcasted_iota(jnp.int32, score.shape, 1)
                score = jnp.where(key <= query, score, -1e30)
            old = peak[h : h + 1, :]
            new = jnp.maximum(old, jnp.max(score, axis=0, keepdims=True))
            expo = jnp.exp2(score - new)
            factor = jnp.exp2(old - new)
            peak[h : h + 1, :] = new
            total[h : h + 1, :] = total[h : h + 1, :] * factor + jnp.sum(
                expo, axis=0, keepdims=True
            )
            part_rows = slice(h * vdim, (h + 1) * vdim)
            acc[part_rows, :] = acc[part_rows, :] * factor + jnp.dot(
                vals[part_rows, :], expo.astype(jnp.bfloat16), preferred_element_type=jnp.float32
            )

    @scoped("attend_own")
    def attend_own():
        attend_block(ep, True)

    @scoped("attend_side")
    def attend_side():
        @pl.when(ep % 2 == 1)
        def _():
            attend_block(ep - 1, False)

    @scoped("attend_level")
    def attend_level(k):
        @pl.when(level >= k)
        def _():
            @pl.loop(0, 2)
            def _(side):
                attend_block((level - k) * 2 + side, False)

    @scoped("combine")
    def combine(s):
        if s:
            to_home(s).wait_recv()
        group = partner(ep, s)
        both = lax.dot_general(
            shares[group],
            back[group],
            (((0,), (0,)), ((), ())),
            preferred_element_type=jnp.float32,
        )
        blend[...] += both[:rows] + both[rows:]

    @scoped("attend_end")
    def attend_end():
        for h in range(heads):
            part_rows = slice(h * vdim, (h + 1) * vdim)
            attended[:, part_rows] = (acc[part_rows, :] / total[h : h + 1, :]).T.astype(
                jnp.bfloat16
            )

    @scoped("mix")
    def mix(owner_y, owner_core):
        start = pl.multiple_of((owner_y * 2 + owner_core) * rows, rows)
        return jnp.dot(
            attended[pl.ds(start, rows), :], output_w[...], preferred_element_type=jnp.float32
        ).astype(jnp.bfloat16)

    mix_near = box.copy(mixed.at[2:4], mix_sib, mix_sem, 0, tp=1)
    mix_over = box.copy(mix_chip, mix_far, mix_sem, 1, tp=2)

    own_copy = pltpu.make_async_copy(outgoing.at[ep], recv.at[0, 0], load_sem.at[9])
    lat_over.start()
    lat_near.start()
    q_over.start()
    q_near.start()
    loads[3].wait()
    scope = jax.named_scope("prepare_rows")
    scope.__enter__()
    prepare_rows(
        local,
        main,
        rest,
        rows_in,
        moe_gain,
        routes,
        route_weight,
        outgoing,
        shares,
    )
    scope.__exit__(None, None, None)
    own_copy.start()
    quarter = groups // 4
    outer = range(quarter, steps)
    inner = range(1, quarter)
    for s in range(1, 2 * quarter + 2):
        dispatch(s).start()
    forward(0)
    lat_over.wait_recv()
    lat_near_over.start()
    chain(0)
    for s in range(2 * quarter + 2, groups):
        dispatch(s).start()
    forward(1)
    for one in loads[4:] + loads[:3] + [own_copy]:
        one.wait()
    q_over.wait_recv()
    q_near_over.start()
    cross(0)
    attend_start()
    blend[...] = jnp.zeros_like(blend)
    for s in range(2, 2 * quarter):
        forward(s)
    q_near.wait_recv()
    q_near_over.wait_recv()
    project_queries()
    cross(1)
    compute(0)
    forward(2 * quarter)
    forward(2 * quarter + 1)
    chain_side(0)
    chain(1)
    for k in inner:
        cross(2 * k)
        cross(2 * k + 1)
        compute(k)
    lat_near.wait_recv()
    lat_near_over.wait_recv()
    attend_own()
    for k in outer:
        for s in (2 * k + 2, 2 * k + 3):
            if s < groups:
                forward(s)
        number = k - quarter + 1
        cross(2 * k)
        cross(2 * k + 1)
        compute(k)
        chain_side(number)
        if number + 1 < levels:
            chain(number + 1)
        chip_sum(k)
        if k == quarter:
            chain_end(0)
            attend_side()
            for one in (0, *inner):
                chip_sum(one)
    for k in (0, *inner):
        for s in (2 * k, 2 * k + 1):
            to_far(s).start()
    chain_end(1)
    attend_level(1)
    for number, k in enumerate(outer):
        finish(k)
        if number + 2 < levels:
            if number + 2 > len(outer):
                chain_side(number + 2)
            chain_end(number + 2)
            attend_level(number + 2)
    for number in range(len(outer) + 2, levels):
        chain_side(number)
        chain_end(number)
        attend_level(number)
    attend_end()
    mixed[2] = mix(y, 1 - core)
    mixed[3] = mix(1 - y, 1 - core)
    mix_near.start()
    mixed[0] = mix(y, core)
    mixed[1] = mix(1 - y, core)
    mix_near.wait_recv()
    mix_chip[...] = add_rounded(mixed[1], mix_sib[1])
    mix_over.start()
    mixed[0] = add_rounded(mixed[0], mix_sib[0])
    for k in (0, *inner):
        finish(k)
    combine(0)
    for k in outer:
        combine(2 * k)
        combine(2 * k + 1)
    combine(1)
    for s in range(2, 2 * quarter):
        combine(s)
    mix_over.wait_recv()
    mixed_out[...] = mixed[0].astype(jnp.float32) + mix_far[...].astype(jnp.float32)
    expert_out[...] = blend[...]
    for s in range(1, groups):
        dispatch(s).wait_send()
        to_home(s).wait_send()
    for s in range(groups):
        to_far(s).wait_send()
    for k in range(steps):
        to_part(k).wait_send()
    for one in (lat_over, lat_near, lat_near_over, q_over, q_near, q_near_over, mix_near, mix_over):
        one.wait_send()


def fused(groups, small, rows_in, weights, sizes):
    heads, rope, main, rest = sizes
    query_in, kv_in = small[0], small[1]
    gate_w, up_w, down_w = weights[-3:]
    depth = rows_in.shape[1]
    rows, kv_width = kv_in.shape
    local = gate_w.shape[0]
    piece = local * (main + rest)
    vdims = weights[3].shape[1]
    chunks = 8
    mains = chunks * main
    rests = chunks * local * rest
    bf, fl = jnp.bfloat16, jnp.float32
    vmem = pl.BlockSpec(memory_space=pltpu.VMEM)
    hbm = pl.BlockSpec(memory_space=pl.ANY)
    levels = groups // 2
    sem = pltpu.SemaphoreType.DMA
    scratch = [
        pltpu.VMEM(rows_in.shape, bf),
        pltpu.VMEM((groups, piece, depth), bf),
        pltpu.VMEM((groups, piece, depth), bf),
        pltpu.VMEM((groups, piece, 2 * rows), bf),
        pltpu.VMEM(rows_in.shape, fl),
        *[pltpu.VMEM(one.shape, bf) for one in weights[:-3]],
        pltpu.VMEM((vdims, kv_width), bf),
        pltpu.VMEM((4 * rows, heads * PAD), bf),
        *[pltpu.VMEM(one.shape, bf) for one in weights[-3:]],
        pltpu.VMEM((groups, 4, piece, depth), bf),
        pltpu.VMEM((groups, 2, piece, depth), bf),
        pltpu.VMEM((groups, piece, depth), bf),
        pltpu.VMEM((groups, piece, depth), bf),
        pltpu.VMEM((groups, piece, depth), bf),
        pltpu.VMEM((mains + rests, depth), bf),
        pltpu.VMEM((rests, depth), fl),
        pltpu.VMEM((groups, 2, 2, rows, kv_width + rope), bf),
        pltpu.VMEM((rows, 2 * rope), fl),
        pltpu.VMEM((2, 2) + query_in.shape, bf),
        pltpu.VMEM((4 * rows, heads * PAD), bf),
        pltpu.VMEM((heads, 4 * rows), fl),
        pltpu.VMEM((heads, 4 * rows), fl),
        pltpu.VMEM((vdims, 4 * rows), fl),
        pltpu.VMEM((4 * rows, vdims), bf),
        pltpu.VMEM((4, rows, depth), bf),
        pltpu.VMEM((2, rows, depth), bf),
        pltpu.VMEM((rows, depth), bf),
        pltpu.VMEM((rows, depth), bf),
        sem((10,)),
        sem((2, groups)),
        sem((2, groups)),
        sem((2, groups)),
        sem((2, groups)),
        sem((2, groups // 2)),
        sem((2, groups)),
        sem((2, groups)),
        sem((2, 3)),
        sem((2, levels)),
        sem((2, levels)),
        sem((2, levels)),
        sem((2, levels)),
        sem((2, 3)),
        sem((2, 2)),
    ]
    return pl.pallas_call(
        functools.partial(fused_kernel, heads, rope, main, rest),
        out_shape=(
            jax.ShapeDtypeStruct((rows, depth), fl),
            jax.ShapeDtypeStruct((rows, depth), fl),
        ),
        in_specs=[vmem] * len(small) + [hbm] * (1 + len(weights)),
        out_specs=(vmem, vmem),
        scratch_shapes=scratch,
        compiler_params=pltpu.CompilerParams(
            collective_id=0, has_side_effects=True, vmem_limit_bytes=62 * 1024 * 1024
        ),
    )(*small, rows_in, *weights)


def per_device(
    query_latent,
    kv_latent,
    rope_key,
    query_gain,
    kv_gain,
    query_nope_w,
    query_rope_w,
    key_up_w,
    value_up_w,
    output_w,
    expert_in,
    moe_gain,
    routes,
    route_weight,
    gate_w,
    up_w,
    down_w,
):
    tok_rows, top_count = routes.shape
    width = expert_in.shape[1]
    local = gate_w.shape[0]
    rope = rope_key.shape[1]
    heads = query_nope_w.shape[1] // NOPE
    ep_size, tp_size = lax.axis_size("ep"), lax.axis_size("tp")
    experts = local * ep_size
    capacity = max(2, 5 * tok_rows * top_count // (4 * experts))
    main = capacity // 8 * 8
    rest = capacity - main
    if not (
        tp_size == 4
        and ep_size & (ep_size - 1) == 0
        and main % 16 == 0
        and local * rest % 8 == 0
        and heads * rope == 128
        and 2 * rope == 128
        and ep_size >= 4
    ):
        return plain_device(
            query_latent,
            kv_latent,
            rope_key,
            query_gain,
            kv_gain,
            query_nope_w,
            query_rope_w,
            key_up_w,
            value_up_w,
            output_w,
            expert_in,
            moe_gain,
            routes,
            route_weight,
            gate_w,
            up_w,
            down_w,
        )
    half = rope // 2
    exponent = np.arange(half, dtype=np.float32) * np.float32(2.0) / np.float32(rope)
    freq = np.float32(1.0) / np.float32(THETA) ** exponent
    small = (
        query_latent,
        kv_latent,
        rope_key.T,
        query_gain,
        kv_gain,
        jnp.asarray(np.tile(freq, 4)[None, :]),
        moe_gain,
        routes.T,
        route_weight.T,
    )
    big = (query_nope_w, query_rope_w, key_up_w, value_up_w, output_w, gate_w, up_w, down_w)
    mixed, blend = fused(ep_size, small, expert_in, big, (heads, rope, main, rest))
    return mixed.astype(jnp.bfloat16), blend.astype(jnp.bfloat16)


def solution(mesh):
    placed = (
        P(("ep", "tp"), None),
        P(("ep", "tp"), None),
        P(("ep", "tp"), None),
        P(),
        P(),
        P(None, "tp"),
        P(None, "tp"),
        P(None, "tp"),
        P(None, "tp"),
        P("tp", None),
        P(("ep", "tp"), None),
        P(),
        P(("ep", "tp"), None),
        P(("ep", "tp"), None),
        P("ep", None, "tp"),
        P("ep", None, "tp"),
        P("ep", "tp", None),
    )
    return jax.shard_map(
        per_device,
        mesh=mesh,
        in_specs=placed,
        out_specs=(P(("ep", "tp"), None), P(("ep", "tp"), None)),
        check_vma=False,
    )
```

```python
import functools
import math

import jax
import jax.numpy as jnp
import numpy as np
from jax import lax
from jax.experimental import pallas as pl
from jax.experimental.pallas import tpu as pltpu
from jax.sharding import PartitionSpec as P

NOPE = 128


THETA = 10000.0

PAD = 256

NT = (((1,), (1,)), ((), ()))


def rms_scale(values, gain):
    floats = values.astype(jnp.float32)
    square = jnp.mean(floats * floats, axis=-1, keepdims=True)
    return (floats * lax.rsqrt(square + 1e-06) * gain).astype(jnp.bfloat16)


def attend_kernel(heads, rope, last_ref, lat_ref, q_ref, wk_ref, wv_ref, out_ref, peak, total, acc):
    rows = q_ref.shape[0]
    vdim = wv_ref.shape[0] // heads
    scale = math.log2(math.e) / math.sqrt(NOPE + rope)
    peak[...] = jnp.full_like(peak, -1e30)
    total[...] = jnp.zeros_like(total)
    acc[...] = jnp.zeros_like(acc)

    def block(number, masked):
        lat = lat_ref[pl.ds(pl.multiple_of(number * rows, rows), rows), :]
        keys = jnp.dot(lat, wk_ref[...], preferred_element_type=jnp.float32).astype(jnp.bfloat16)
        vals = lax.dot_general(
            wv_ref[...], lat, NT, preferred_element_type=jnp.float32
        ).astype(jnp.bfloat16)
        for h in range(heads):
            score = (
                lax.dot_general(
                    keys[:, h * PAD : (h + 1) * PAD],
                    q_ref[:, h * PAD : (h + 1) * PAD],
                    NT,
                    preferred_element_type=jnp.float32,
                )
                * scale
            )
            if masked:
                key = lax.broadcasted_iota(jnp.int32, score.shape, 0)
                query = lax.broadcasted_iota(jnp.int32, score.shape, 1)
                score = jnp.where(key <= query, score, -1e30)
            old = peak[h : h + 1, :]
            new = jnp.maximum(old, jnp.max(score, axis=0, keepdims=True))
            expo = jnp.exp2(score - new)
            factor = jnp.exp2(old - new)
            peak[h : h + 1, :] = new
            total[h : h + 1, :] = total[h : h + 1, :] * factor + jnp.sum(
                expo, axis=0, keepdims=True
            )
            part = slice(h * vdim, (h + 1) * vdim)
            acc[part, :] = acc[part, :] * factor + jnp.dot(
                vals[part, :], expo.astype(jnp.bfloat16), preferred_element_type=jnp.float32
            )

    last = last_ref[0]

    @pl.loop(0, last)
    def _(number):
        block(number, False)

    block(last, True)
    for h in range(heads):
        part = slice(h * vdim, (h + 1) * vdim)
        out_ref[part, :] = (acc[part, :] / total[h : h + 1, :]).astype(jnp.bfloat16)


def attend(last, latents, queries, key_w, value_w, heads, rope):
    rows = queries.shape[0]
    vdim_all = value_w.shape[0]
    vmem = pl.BlockSpec(memory_space=pltpu.VMEM)
    length = latents.shape[0]
    return pl.pallas_call(
        functools.partial(attend_kernel, heads, rope),
        out_shape=jax.ShapeDtypeStruct((vdim_all, rows), jnp.bfloat16),
        in_specs=[pl.BlockSpec(memory_space=pltpu.SMEM)] + [vmem] * 4,
        out_specs=vmem,
        scratch_shapes=[
            pltpu.VMEM((heads, rows), jnp.float32),
            pltpu.VMEM((heads, rows), jnp.float32),
            pltpu.VMEM((vdim_all, rows), jnp.float32),
        ],
        compiler_params=pltpu.CompilerParams(vmem_limit_bytes=40 * 1024 * 1024),
        cost_estimate=pl.CostEstimate(
            flops=2 * length * rows * heads * (PAD + 2 * NOPE),
            bytes_accessed=latents.size * 2,
            transcendentals=length * rows * heads,
        ),
    )(last, latents, queries, key_w, value_w)


def mixer_front(query_latent, kv_latent, rope_key, query_gain, kv_gain):
    tok_rows = query_latent.shape[0]
    rope = rope_key.shape[1]
    half = rope // 2
    group_rows = tok_rows * lax.axis_size("tp")
    freq = 1.0 / THETA ** (jnp.arange(half, dtype=jnp.float32) * 2.0 / rope)
    first_pos = lax.axis_index("ep") * group_rows
    positions = first_pos + jnp.arange(group_rows, dtype=jnp.int32)
    own = lax.axis_index("tp") * tok_rows + first_pos + jnp.arange(tok_rows, dtype=jnp.int32)
    angle = own.astype(jnp.float32)[:, None] * jnp.tile(freq, 2)[None, :]
    keys = rope_key.astype(jnp.float32)
    turned = jnp.concatenate([-keys[:, half:], keys[:, :half]], axis=-1)
    key_rot = (keys * jnp.cos(angle) + turned * jnp.sin(angle)).astype(jnp.bfloat16)
    kv_normed = rms_scale(kv_latent, kv_gain)
    own_latents = jnp.concatenate([kv_normed, key_rot], axis=1)
    query_normed = lax.all_gather(rms_scale(query_latent, query_gain), "tp", axis=0, tiled=True)
    return own_latents, query_normed, positions, freq


def mixer(
    front, rope, query_nope_w, query_rope_w, key_up_w, value_up_w, output_w
):
    latents, query_normed, positions, freq = front
    half = rope // 2
    heads = query_nope_w.shape[1] // NOPE
    kv_width = key_up_w.shape[0]
    angle = positions.astype(jnp.float32)[:, None] * jnp.tile(freq, 2 * heads)[None, :]
    turned_w = []
    for h in range(heads):
        turned_w.append(-query_rope_w[:, h * rope + half : (h + 1) * rope])
        turned_w.append(query_rope_w[:, h * rope : h * rope + half])
    weights = jnp.concatenate([query_nope_w, query_rope_w] + turned_w, axis=1)
    flat = jnp.dot(query_normed, weights, preferred_element_type=jnp.float32)
    nope_all = heads * NOPE
    rope_all = heads * rope
    rot = (
        flat[:, nope_all : nope_all + rope_all] * jnp.cos(angle)
        + flat[:, nope_all + rope_all :] * jnp.sin(angle)
    ).astype(jnp.bfloat16)
    query_flat = flat[:, :nope_all].astype(jnp.bfloat16)
    blank = jnp.zeros((flat.shape[0], PAD - NOPE - rope), jnp.bfloat16)
    pieces = []
    for h in range(heads):
        pieces += [
            query_flat[:, h * NOPE : (h + 1) * NOPE],
            rot[:, h * rope : (h + 1) * rope],
            blank,
        ]
    queries = jnp.concatenate(pieces, axis=1)
    carry = jnp.pad(
        jnp.eye(rope, dtype=jnp.bfloat16), ((0, 0), (NOPE, PAD - NOPE - rope))
    )
    key_w = jnp.concatenate(
        [
            jnp.concatenate(
                [
                    jnp.pad(key_up_w[:, h * NOPE : (h + 1) * NOPE], ((0, 0), (0, PAD - NOPE))),
                    carry,
                ],
                axis=0,
            )
            for h in range(heads)
        ],
        axis=1,
    )
    value_w = jnp.pad(value_up_w.T, ((0, 0), (0, latents.shape[1] - kv_width)))
    last = lax.axis_index("ep").astype(jnp.int32).reshape(1)
    attended = attend(last, latents, queries, key_w, value_w, heads, rope)
    mixed = lax.dot_general(
        attended, output_w, (((0,), (0,)), ((), ())), preferred_element_type=jnp.float32
    ).astype(jnp.bfloat16)
    return lax.psum_scatter(mixed, "tp", scatter_dimension=0, tiled=True)


def route(routes, experts, local, capacity):
    rows = routes.shape[0]
    main = capacity // 8 * 8
    rest = capacity - main
    names = jnp.arange(experts, dtype=jnp.int32)[None, :]
    chosen = [routes[:, k : k + 1] == names for k in range(routes.shape[1])]
    member = functools.reduce(jnp.logical_or, chosen).astype(jnp.bfloat16)
    before = lax.broadcasted_iota(jnp.int32, (rows, rows), 0) > lax.broadcasted_iota(
        jnp.int32, (rows, rows), 1
    )
    rank = jnp.dot(
        before.astype(jnp.bfloat16), member, preferred_element_type=jnp.float32
    ).astype(jnp.int32)
    inner = names % local
    place = jnp.where(
        rank < main, inner * main + rank, local * main + inner * rest + rank - main
    ) + names // local * (local * capacity)
    slots = lax.broadcasted_iota(jnp.int32, (rows, experts * capacity), 1)
    return [
        jnp.sum(jnp.where(one, place, 0), axis=1, keepdims=True) == slots for one in chosen
    ]


def swap(values, bit):
    size = lax.axis_size("tp")
    return lax.ppermute(values, "tp", [(one, one ^ bit) for one in range(size)])


def expert_rows(pieces, local, main, rest, gate_w, up_w, down_w):
    groups, piece, width = pieces.shape
    mixed = pieces[:, local * main :].reshape(groups * local * rest, width)
    owner = (
        lax.broadcasted_iota(jnp.int32, (groups * local * rest, 1), 0) % (local * rest)
    ) // max(rest, 1)
    mains = []
    shared = 0.0
    for expert in range(local):
        inputs = jnp.concatenate(
            [
                pieces[:, expert * main : (expert + 1) * main].reshape(groups * main, width),
                mixed,
            ],
            axis=0,
        )
        gate = jnp.minimum(jnp.dot(inputs, gate_w[expert], preferred_element_type=jnp.float32), 7.0)
        upper = jnp.clip(
            jnp.dot(inputs, up_w[expert], preferred_element_type=jnp.float32), -7.0, 7.0
        )
        hidden = (gate * jax.nn.sigmoid(1.702 * gate) * (upper + 1.0)).astype(jnp.bfloat16)
        output = jnp.dot(hidden, down_w[expert], preferred_element_type=jnp.float32).astype(
            jnp.bfloat16
        )
        mains.append(output[: groups * main].reshape(groups, main, width))
        shared = jnp.where(owner == expert, output[groups * main :], shared)
    shared = shared.astype(jnp.bfloat16).reshape(groups, local * rest, width)
    return jnp.concatenate(mains + [shared], axis=1)


def add_rounded(one, other):
    return (one.astype(jnp.float32) + other.astype(jnp.float32)).astype(jnp.bfloat16)


def group_experts(arrived, run):
    size = lax.axis_size("tp")
    if size & (size - 1):
        spread = lax.all_gather(arrived, "tp", axis=0, tiled=True)
        return lax.psum_scatter(run(spread), "tp", scatter_dimension=0, tiled=True)
    count = arrived.shape[0]
    far = {0: arrived}
    for bit in [1 << k for k in range(1, size.bit_length() - 1)]:
        for key in sorted(far):
            far[key | bit] = swap(far[key], bit)
    results = {}
    for key in sorted(far):
        if size == 1:
            results[key] = run(far[key])
            continue
        near = swap(far[key], 1)
        both = run(jnp.concatenate([far[key], near], axis=0))
        results[key] = add_rounded(both[:count], swap(both[count:], 1))
    for bit in [1 << k for k in range(size.bit_length() - 2, 0, -1)]:
        for key in sorted(results):
            if key & bit:
                results[key ^ bit] = add_rounded(results[key ^ bit], swap(results.pop(key), bit))
    return results[0]


def experts_half(expert_in, moe_gain, routes, route_weight, gate_w, up_w, down_w, tied):
    tok_rows, top_count = routes.shape
    width = expert_in.shape[1]
    local = gate_w.shape[0]
    ep_size = lax.axis_size("ep")
    experts = local * ep_size
    capacity = max(2, 5 * tok_rows * top_count // (4 * experts))
    main = capacity // 8 * 8
    rest = capacity - main
    piece = local * capacity
    floats = expert_in.astype(jnp.float32)
    center = floats - jnp.mean(floats, axis=-1, keepdims=True)
    variance = jnp.mean(center * center, axis=-1, keepdims=True)
    normed_in = (center * lax.rsqrt(variance + 1e-05) * moe_gain).astype(jnp.bfloat16)
    hits = route(routes, experts, local, capacity)
    select = functools.reduce(jnp.logical_or, hits).astype(jnp.bfloat16)
    outgoing = lax.dot_general(
        select, normed_in, (((0,), (0,)), ((), ())), preferred_element_type=jnp.float32
    ).astype(jnp.bfloat16)
    outgoing, tied = lax.optimization_barrier((outgoing, tied))
    latents = lax.all_gather(tied, ("ep", "tp"), axis=0, tiled=True)
    outgoing = outgoing.reshape(ep_size, piece, width)
    arrived = lax.all_to_all(outgoing, "ep", split_axis=0, concat_axis=0, tiled=True)
    summed = group_experts(
        arrived,
        lambda pieces: expert_rows(pieces, local, main, rest, gate_w, up_w, down_w),
    )
    back = lax.all_to_all(summed, "ep", split_axis=0, concat_axis=0, tiled=True).reshape(
        experts * capacity, width
    )
    weights = route_weight / jnp.sum(route_weight, axis=-1, keepdims=True)
    mix = sum(jnp.where(hit, weights[:, k : k + 1], 0.0) for k, hit in enumerate(hits))
    high = mix.astype(jnp.bfloat16)
    low = (mix - high.astype(jnp.float32)).astype(jnp.bfloat16)
    both = jnp.dot(
        jnp.concatenate([high, low], axis=0), back, preferred_element_type=jnp.float32
    )
    return (both[:tok_rows] + both[tok_rows:]).astype(jnp.bfloat16), latents


def plain_device(
    query_latent,
    kv_latent,
    rope_key,
    query_gain,
    kv_gain,
    query_nope_w,
    query_rope_w,
    key_up_w,
    value_up_w,
    output_w,
    expert_in,
    moe_gain,
    routes,
    route_weight,
    gate_w,
    up_w,
    down_w,
):
    front = mixer_front(query_latent, kv_latent, rope_key, query_gain, kv_gain)
    expert_out, latents = experts_half(
        expert_in, moe_gain, routes, route_weight, gate_w, up_w, down_w, front[0]
    )
    mixer_out = mixer(
        (latents,) + front[1:],
        rope_key.shape[1],
        query_nope_w,
        query_rope_w,
        key_up_w,
        value_up_w,
        output_w,
    )
    return (mixer_out, expert_out)


MESH = pl.DeviceIdType.MESH


def partner(index, bits):
    place = 1
    while place <= bits:
        if bits & place:
            index = index + place * (1 - 2 * ((index // place) % 2))
        place *= 2
    return index


def scoped(name):
    def wrap(inner):
        def run(*args):
            with jax.named_scope(name + "".join(str(a) for a in args if isinstance(a, int))):
                return inner(*args)

        return run

    return wrap


class Mail:
    def __init__(self, ep, tp):
        self.ep, self.tp, self.sent = ep, tp, []

    def copy(self, source, target, sems, number, ep=0, tp=0, up=0):
        return pltpu.make_async_remote_copy(
            src_ref=source,
            dst_ref=target,
            send_sem=sems.at[0, number],
            recv_sem=sems.at[1, number],
            device_id=(partner(self.ep, ep) + up, partner(self.tp, tp)),
            device_id_type=MESH,
        )


def expert_step(step, main, rest, recv, lhs, held, gate_w, up_w, down_w):
    local = gate_w.shape[0]
    depth = lhs.shape[1]
    chunks = recv.shape[1] * 2
    mains = chunks * main
    rests = chunks * local * rest
    span = slice(2 * step, 2 * step + 2)
    tail = slice(local * main, local * (main + rest))
    lhs[mains : mains + rests, :] = (
        recv[span, :, tail, :].astype(jnp.float32).reshape(rests, depth).astype(jnp.bfloat16)
    )
    wide = 512

    if True:
        for a in range(local):
            own = slice(a * main, (a + 1) * main)
            lhs[:mains, :] = recv[span, :, own, :].reshape(mains, depth)
            gate = jnp.minimum(
                jnp.dot(lhs[...], gate_w[a], preferred_element_type=jnp.float32), 7.0
            )
            upper = jnp.clip(
                jnp.dot(lhs[...], up_w[a], preferred_element_type=jnp.float32), -7.0, 7.0
            )
            hidden = (gate * jax.nn.sigmoid(1.702 * gate) * (upper + 1.0)).astype(jnp.bfloat16)
            for first in range(0, depth, wide):
                cols = slice(first, first + wide)
                out = jnp.dot(hidden, down_w[a, :, cols], preferred_element_type=jnp.float32)
                recv[span, :, own, cols] = (
                    out[:mains].astype(jnp.bfloat16).reshape(2, chunks // 2, main, wide)
                )
                if a == 0:
                    held[:, cols] = out[mains:]
                else:
                    row = lax.broadcasted_iota(jnp.int32, (rests, wide), 0) % (local * rest)
                    picked = jnp.where(row // rest == a, out[mains:], held[:, cols])
                    if a < local - 1:
                        held[:, cols] = picked
                    else:
                        recv[span, :, tail, cols] = picked.reshape(
                            2, chunks // 2, local * rest, wide
                        ).astype(jnp.bfloat16)


def prepare_rows(local, main, rest, rows_in, moe_gain, routes, route_weight, outgoing, shares):
    groups, piece, depth = outgoing.shape
    rows = rows_in.shape[0]
    experts = groups * local
    floats = rows_in[...].astype(jnp.float32)
    center = floats - jnp.mean(floats, axis=-1, keepdims=True)
    variance = jnp.mean(center * center, axis=-1, keepdims=True)
    normed = (center * lax.rsqrt(variance + 1e-05) * moe_gain[...][None, :]).astype(jnp.bfloat16)
    chosen = [routes[k : k + 1, :] for k in range(routes.shape[0])]
    names = lax.broadcasted_iota(jnp.int32, (experts, rows), 0)
    match = [one == names for one in chosen]
    member = jnp.where(functools.reduce(jnp.logical_or, match), 1.0, 0.0).astype(jnp.bfloat16)
    before = lax.broadcasted_iota(jnp.int32, (rows, rows), 0) < lax.broadcasted_iota(
        jnp.int32, (rows, rows), 1
    )
    rank = jnp.dot(
        member, jnp.where(before, 1.0, 0.0).astype(jnp.bfloat16), preferred_element_type=jnp.float32
    )
    inner = (names % local).astype(jnp.float32)
    start = ((names // local) * piece).astype(jnp.float32)
    place = start + jnp.where(
        rank < main, inner * main + rank, local * main + inner * rest + rank - main
    )
    places = [
        jnp.sum(jnp.where(one, place, 0.0), axis=0, keepdims=True).astype(jnp.int32)
        for one in match
    ]
    slots = lax.broadcasted_iota(jnp.int32, (groups * piece, rows), 0)
    hits = [one == slots for one in places]
    select = jnp.where(functools.reduce(jnp.logical_or, hits), 1.0, 0.0).astype(jnp.bfloat16)
    outgoing[...] = (
        jnp.dot(select, normed, preferred_element_type=jnp.float32)
        .reshape(groups, piece, depth)
        .astype(jnp.bfloat16)
    )
    loads = [route_weight[k : k + 1, :] for k in range(routes.shape[0])]
    whole = sum(loads)
    share = sum(jnp.where(hit, one / whole, 0.0) for hit, one in zip(hits, loads))
    high = share.astype(jnp.bfloat16).astype(jnp.float32)
    shares[:, :, :rows] = high.reshape(groups, piece, rows).astype(jnp.bfloat16)
    shares[:, :, rows:] = (share - high).reshape(groups, piece, rows).astype(jnp.bfloat16)


def fused_kernel(
    heads,
    rope,
    main,
    rest,
    query_in,
    kv_in,
    rope_in,
    query_gain,
    kv_gain,
    freq,
    moe_gain,
    routes,
    route_weight,
    rows_h,
    nope_h,
    rope_h,
    key_h,
    value_h,
    output_h,
    gate_h,
    up_h,
    down_h,
    mixed_out,
    expert_out,
    rows_in,
    outgoing,
    back,
    shares,
    blend,
    nope_w,
    rope_w,
    key_w,
    value_w,
    output_w,
    value_t,
    keys_s,
    gate_w,
    up_w,
    down_w,
    recv,
    sibling,
    chip,
    far,
    done,
    lhs,
    held,
    lat,
    wide_key,
    queries,
    heads_q,
    peak,
    total,
    acc,
    attended,
    mixed,
    mix_sib,
    mix_chip,
    mix_far,
    load_sem,
    go,
    near_a,
    near_b,
    over,
    part,
    ret,
    home,
    lat_sem,
    chain_up,
    chain_sib,
    chain_x,
    chain_xs,
    q_sem,
    mix_sem,
):
    groups = outgoing.shape[0]
    local = gate_w.shape[0]
    levels = groups // 2
    steps = groups // 2
    rows = kv_in.shape[0]
    kv_width = kv_in.shape[1]
    ep, tp = lax.axis_index("ep"), lax.axis_index("tp")
    half = rope // 2
    level, y, core = ep // 2, tp // 2, tp % 2
    box = Mail(ep, tp)

    loads = [
        pltpu.make_async_copy(gate_h, gate_w, load_sem.at[0]),
        pltpu.make_async_copy(up_h, up_w, load_sem.at[1]),
        pltpu.make_async_copy(down_h, down_w, load_sem.at[2]),
        pltpu.make_async_copy(rows_h, rows_in, load_sem.at[3]),
        pltpu.make_async_copy(nope_h, nope_w, load_sem.at[4]),
        pltpu.make_async_copy(rope_h, rope_w, load_sem.at[5]),
        pltpu.make_async_copy(key_h, key_w, load_sem.at[6]),
        pltpu.make_async_copy(value_h, value_w, load_sem.at[7]),
        pltpu.make_async_copy(output_h, output_w, load_sem.at[8]),
    ]
    for one in loads[3:] + loads[:3]:
        one.start()

    barrier = pltpu.get_barrier_semaphore()
    for bits in range(1, groups):
        pl.semaphore_signal(
            barrier, inc=1, device_id=(partner(ep, bits), tp), device_id_type=MESH
        )
    for bits in (1, 2):
        pl.semaphore_signal(
            barrier, inc=1, device_id=(ep, partner(tp, bits)), device_id_type=MESH
        )
    lane = lax.broadcasted_iota(jnp.int32, (rows, 128), 1)
    place = lax.broadcasted_iota(jnp.int32, (rows, 128), 0) + lane // half * rows
    angle = (place + ep * (4 * rows)).astype(jnp.float32) * freq[...]
    cos_all, sin_all = jnp.cos(angle), jnp.sin(angle)

    def spread(table, block):
        own = jnp.where(lane // half == block, table, 0.0)
        own = own + pltpu.roll(own, half, 1)
        return own + pltpu.roll(own, 2 * half, 1)

    def rotate(values, block):
        turned = jnp.where(
            lane % rope < half, -pltpu.roll(values, 128 - half, 1), pltpu.roll(values, half, 1)
        )
        return values * spread(cos_all, block) + turned * spread(sin_all, block)

    scope = jax.named_scope("latents")
    scope.__enter__()
    lat[ep, y, core, :, :kv_width] = rms_scale(kv_in[...], kv_gain[...][None, :])
    raw_key = rope_in[...].astype(jnp.float32).T
    wide_key[:, :rope] = raw_key
    wide_key[:, rope:] = raw_key
    lat[ep, y, core, :, kv_width:] = rotate(wide_key[...], tp)[:, :rope].astype(jnp.bfloat16)
    queries[y, core] = rms_scale(query_in[...], query_gain[...][None, :])
    scope.__exit__(None, None, None)
    with jax.named_scope("barrier"):
        pl.semaphore_wait(barrier, groups + 1)

    def dispatch(s):
        return box.copy(outgoing.at[partner(ep, s)], recv.at[s, 0], go, s, ep=s)

    def first(s):
        return outgoing.at[ep] if s == 0 else recv.at[s, 0]

    def to_over(s):
        return box.copy(first(s), recv.at[s, 1], over, s, tp=2)

    def to_near(s):
        return box.copy(first(s), recv.at[s, 2], near_a, s, tp=1)

    def to_near_over(s):
        return box.copy(recv.at[s, 1], recv.at[s, 3], near_b, s, tp=1)

    def to_part(k):
        return box.copy(
            recv.at[2 * k : 2 * k + 2, 2:4], sibling.at[2 * k : 2 * k + 2], part, k, tp=1
        )

    def to_far(s):
        return box.copy(chip.at[s], far.at[s], ret, s, tp=2)

    def to_home(s):
        return box.copy(done.at[s], back.at[ep], home, s, ep=s)

    @scoped("forward")
    def forward(s):
        if s:
            dispatch(s).wait_recv()
        to_over(s).start()
        to_near(s).start()

    @scoped("cross")
    def cross(s):
        to_over(s).wait_recv()
        to_near_over(s).start()

    @scoped("compute")
    def compute(k):
        for s in (2 * k, 2 * k + 1):
            to_near(s).wait_recv()
            to_near_over(s).wait_recv()
            to_over(s).wait_send()
            to_near(s).wait_send()
            to_near_over(s).wait_send()
        with jax.named_scope(f"expert{k}"):
            expert_step(k, main, rest, recv, lhs, held, gate_w, up_w, down_w)
        to_part(k).start()

    @scoped("chip_sum")
    def chip_sum(k):
        to_part(k).wait_recv()
        for s in (2 * k, 2 * k + 1):
            chip[s] = add_rounded(recv[s, 1], sibling[s, 1])
            if k >= groups // 4:
                to_far(s).start()
            recv[s, 0] = add_rounded(recv[s, 0], sibling[s, 0])

    @scoped("finish")
    def finish(k):
        for s in (2 * k, 2 * k + 1):
            to_far(s).wait_recv()
            if s == 0:
                back[ep] = add_rounded(recv[s, 0], far[s])
            else:
                done[s] = add_rounded(recv[s, 0], far[s])
                to_home(s).start()

    own_block, own_query = lat.at[ep, y, core], queries.at[y, core]
    lat_over = box.copy(own_block, own_block, lat_sem, 0, tp=2)
    lat_near = box.copy(own_block, own_block, lat_sem, 1, tp=1)
    over_block = lat.at[ep, 1 - y, core]
    lat_near_over = box.copy(over_block, over_block, lat_sem, 2, tp=1)
    q_over = box.copy(own_query, own_query, q_sem, 0, tp=2)
    q_near = box.copy(own_query, own_query, q_sem, 1, tp=1)
    q_over_block = queries.at[1 - y, core]
    q_near_over = box.copy(q_over_block, q_over_block, q_sem, 2, tp=1)

    def blocks(group):
        return lat.at[group, :, core]

    def go_up(k):
        own = blocks(ep - 2 * k)
        return box.copy(own, own, chain_up, k, up=2)

    def go_near(k):
        own = blocks(ep - 2 * k)
        return box.copy(own, own, chain_sib, k, tp=1)

    def go_side(k):
        own = blocks(ep - 2 * k)
        return box.copy(own, own, chain_x, k, ep=1)

    def go_side_near(k):
        own = blocks(partner(ep, 1) - 2 * k)
        return box.copy(own, own, chain_xs, k, tp=1)

    @scoped("chain")
    def chain(k):
        @pl.when(level >= k)
        def _():
            if k:
                box.copy(blocks(ep - 2 * k), blocks(ep - 2 * k), chain_up, k - 1, up=2).wait_recv()
                go_near(k).start()
            if k < levels - 1:

                @pl.when(level < levels - 1)
                def _():
                    go_up(k).start()

            go_side(k).start()

    @scoped("chain_side")
    def chain_side(k):
        @pl.when(level >= k)
        def _():
            go_side(k).wait_recv()
            go_side_near(k).start()

    @scoped("chain_end")
    def chain_end(k):
        @pl.when(level >= k)
        def _():
            if k:
                go_near(k).wait_recv()
                go_near(k).wait_send()
            go_side_near(k).wait_recv()
            go_side_near(k).wait_send()
            go_side(k).wait_send()
            if k < levels - 1:

                @pl.when(level < levels - 1)
                def _():
                    go_up(k).wait_send()

    @scoped("project_queries")
    def project_queries():
        for block in range(4):
            source = queries[block // 2, block % 2]
            span = slice(block * rows, (block + 1) * rows)
            flat = jnp.dot(source, nope_w[...], preferred_element_type=jnp.float32)
            rot = rotate(
                jnp.dot(source, rope_w[...], preferred_element_type=jnp.float32), block
            )
            for h in range(heads):
                heads_q[span, h * PAD : h * PAD + NOPE] = flat[
                    :, h * NOPE : (h + 1) * NOPE
                ].astype(jnp.bfloat16)
                shifted = pltpu.roll(rot, 128 - h * rope, 1) if h else rot
                heads_q[span, h * PAD + NOPE : (h + 1) * PAD] = jnp.where(
                    lane < rope, shifted, 0.0
                ).astype(jnp.bfloat16)

    count = 4 * rows
    vdim = value_w.shape[1] // heads
    scale = math.log2(math.e) / math.sqrt(NOPE + rope)

    @scoped("attend_start")
    def attend_start():
        peak[...] = jnp.full_like(peak, -1e30)
        total[...] = jnp.zeros_like(total)
        acc[...] = jnp.zeros_like(acc)
        value_t[...] = value_w[...].astype(jnp.float32).T.astype(jnp.bfloat16)
        for h in range(heads):
            keys_s[:, h * PAD + NOPE : (h + 1) * PAD] = jnp.zeros(
                (count, PAD - NOPE), jnp.bfloat16
            )

    def attend_block(number, masked):
        seen = lat[number, :, :, :, :kv_width].reshape(count, kv_width)
        turned_key = lat[number, :, :, :, kv_width:].reshape(count, rope)
        flat = jnp.dot(seen, key_w[...], preferred_element_type=jnp.float32)
        vals = lax.dot_general(
            value_t[...], seen, NT, preferred_element_type=jnp.float32
        ).astype(jnp.bfloat16)
        for h in range(heads):
            keys_s[:, h * PAD : h * PAD + NOPE] = flat[:, h * NOPE : (h + 1) * NOPE].astype(
                jnp.bfloat16
            )
            keys_s[:, h * PAD + NOPE : h * PAD + NOPE + rope] = turned_key
        for h in range(heads):
            score = (
                lax.dot_general(
                    keys_s[:, h * PAD : (h + 1) * PAD],
                    heads_q[:, h * PAD : (h + 1) * PAD],
                    NT,
                    preferred_element_type=jnp.float32,
                )
                * scale
            )
            if masked:
                key = lax.broadcasted_iota(jnp.int32, score.shape, 0)
                query = lax.broadcasted_iota(jnp.int32, score.shape, 1)
                score = jnp.where(key <= query, score, -1e30)
            old = peak[h : h + 1, :]
            new = jnp.maximum(old, jnp.max(score, axis=0, keepdims=True))
            expo = jnp.exp2(score - new)
            factor = jnp.exp2(old - new)
            peak[h : h + 1, :] = new
            total[h : h + 1, :] = total[h : h + 1, :] * factor + jnp.sum(
                expo, axis=0, keepdims=True
            )
            part_rows = slice(h * vdim, (h + 1) * vdim)
            acc[part_rows, :] = acc[part_rows, :] * factor + jnp.dot(
                vals[part_rows, :], expo.astype(jnp.bfloat16), preferred_element_type=jnp.float32
            )

    @scoped("attend_own")
    def attend_own():
        attend_block(ep, True)

    @scoped("attend_side")
    def attend_side():
        @pl.when(ep % 2 == 1)
        def _():
            attend_block(ep - 1, False)

    @scoped("attend_level")
    def attend_level(k):
        @pl.when(level >= k)
        def _():
            @pl.loop(0, 2)
            def _(side):
                attend_block((level - k) * 2 + side, False)

    @scoped("combine")
    def combine(s):
        if s:
            to_home(s).wait_recv()
        group = partner(ep, s)
        both = lax.dot_general(
            shares[group],
            back[group],
            (((0,), (0,)), ((), ())),
            preferred_element_type=jnp.float32,
        )
        blend[...] += both[:rows] + both[rows:]

    @scoped("attend_end")
    def attend_end():
        for h in range(heads):
            part_rows = slice(h * vdim, (h + 1) * vdim)
            attended[:, part_rows] = (acc[part_rows, :] / total[h : h + 1, :]).T.astype(
                jnp.bfloat16
            )

    @scoped("mix")
    def mix(owner_y, owner_core):
        start = pl.multiple_of((owner_y * 2 + owner_core) * rows, rows)
        return jnp.dot(
            attended[pl.ds(start, rows), :], output_w[...], preferred_element_type=jnp.float32
        ).astype(jnp.bfloat16)

    mix_near = box.copy(mixed.at[2:4], mix_sib, mix_sem, 0, tp=1)
    mix_over = box.copy(mix_chip, mix_far, mix_sem, 1, tp=2)

    own_copy = pltpu.make_async_copy(outgoing.at[ep], recv.at[0, 0], load_sem.at[9])
    lat_over.start()
    lat_near.start()
    q_over.start()
    q_near.start()
    loads[3].wait()
    scope = jax.named_scope("prepare_rows")
    scope.__enter__()
    prepare_rows(
        local,
        main,
        rest,
        rows_in,
        moe_gain,
        routes,
        route_weight,
        outgoing,
        shares,
    )
    scope.__exit__(None, None, None)
    own_copy.start()
    quarter = groups // 4
    outer = range(quarter, steps)
    inner = range(1, quarter)
    for s in range(1, 2 * quarter + 2):
        dispatch(s).start()
    forward(0)
    lat_over.wait_recv()
    lat_near_over.start()
    chain(0)
    for s in range(2 * quarter + 2, groups):
        dispatch(s).start()
    forward(1)
    for one in loads[4:] + loads[:3] + [own_copy]:
        one.wait()
    q_over.wait_recv()
    q_near_over.start()
    cross(0)
    attend_start()
    blend[...] = jnp.zeros_like(blend)
    for s in range(2, 2 * quarter):
        forward(s)
    q_near.wait_recv()
    q_near_over.wait_recv()
    project_queries()
    cross(1)
    compute(0)
    forward(2 * quarter)
    forward(2 * quarter + 1)
    chain_side(0)
    chain(1)
    for k in inner:
        cross(2 * k)
        cross(2 * k + 1)
        compute(k)
    lat_near.wait_recv()
    lat_near_over.wait_recv()
    attend_own()
    for k in outer:
        for s in (2 * k + 2, 2 * k + 3):
            if s < groups:
                forward(s)
        number = k - quarter + 1
        cross(2 * k)
        cross(2 * k + 1)
        compute(k)
        if number == 1:
            for one in (0, *inner):
                chip_sum(one)
        chip_sum(k)
        if number == len(outer):
            for one in (0, *inner):
                for s in (2 * one, 2 * one + 1):
                    to_far(s).start()
        chain_side(number)
        if number + 1 < levels:
            chain(number + 1)
        if number == 1:
            chain_end(0)
            attend_side()
    chain_end(1)
    attend_level(1)
    for number, k in enumerate(outer):
        finish(k)
        if number + 2 < levels:
            if number + 2 > len(outer):
                chain_side(number + 2)
            chain_end(number + 2)
            attend_level(number + 2)
    for number in range(len(outer) + 2, levels):
        chain_side(number)
        chain_end(number)
        attend_level(number)
    attend_end()
    mixed[2] = mix(y, 1 - core)
    mixed[3] = mix(1 - y, 1 - core)
    mix_near.start()
    mixed[0] = mix(y, core)
    mixed[1] = mix(1 - y, core)
    mix_near.wait_recv()
    mix_chip[...] = add_rounded(mixed[1], mix_sib[1])
    mix_over.start()
    mixed[0] = add_rounded(mixed[0], mix_sib[0])
    for k in (0, *inner):
        finish(k)
    combine(0)
    for k in outer:
        combine(2 * k)
        combine(2 * k + 1)
    combine(1)
    for s in range(2, 2 * quarter):
        combine(s)
    mix_over.wait_recv()
    mixed_out[...] = mixed[0].astype(jnp.float32) + mix_far[...].astype(jnp.float32)
    expert_out[...] = blend[...]
    for s in range(1, groups):
        dispatch(s).wait_send()
        to_home(s).wait_send()
    for s in range(groups):
        to_far(s).wait_send()
    for k in range(steps):
        to_part(k).wait_send()
    for one in (lat_over, lat_near, lat_near_over, q_over, q_near, q_near_over, mix_near, mix_over):
        one.wait_send()


def fused(groups, small, rows_in, weights, sizes):
    heads, rope, main, rest = sizes
    query_in, kv_in = small[0], small[1]
    gate_w, up_w, down_w = weights[-3:]
    depth = rows_in.shape[1]
    rows, kv_width = kv_in.shape
    local = gate_w.shape[0]
    piece = local * (main + rest)
    vdims = weights[3].shape[1]
    chunks = 8
    mains = chunks * main
    rests = chunks * local * rest
    bf, fl = jnp.bfloat16, jnp.float32
    vmem = pl.BlockSpec(memory_space=pltpu.VMEM)
    hbm = pl.BlockSpec(memory_space=pl.ANY)
    levels = groups // 2
    sem = pltpu.SemaphoreType.DMA
    scratch = [
        pltpu.VMEM(rows_in.shape, bf),
        pltpu.VMEM((groups, piece, depth), bf),
        pltpu.VMEM((groups, piece, depth), bf),
        pltpu.VMEM((groups, piece, 2 * rows), bf),
        pltpu.VMEM(rows_in.shape, fl),
        *[pltpu.VMEM(one.shape, bf) for one in weights[:-3]],
        pltpu.VMEM((vdims, kv_width), bf),
        pltpu.VMEM((4 * rows, heads * PAD), bf),
        *[pltpu.VMEM(one.shape, bf) for one in weights[-3:]],
        pltpu.VMEM((groups, 4, piece, depth), bf),
        pltpu.VMEM((groups, 2, piece, depth), bf),
        pltpu.VMEM((groups, piece, depth), bf),
        pltpu.VMEM((groups, piece, depth), bf),
        pltpu.VMEM((groups, piece, depth), bf),
        pltpu.VMEM((mains + rests, depth), bf),
        pltpu.VMEM((rests, depth), fl),
        pltpu.VMEM((groups, 2, 2, rows, kv_width + rope), bf),
        pltpu.VMEM((rows, 2 * rope), fl),
        pltpu.VMEM((2, 2) + query_in.shape, bf),
        pltpu.VMEM((4 * rows, heads * PAD), bf),
        pltpu.VMEM((heads, 4 * rows), fl),
        pltpu.VMEM((heads, 4 * rows), fl),
        pltpu.VMEM((vdims, 4 * rows), fl),
        pltpu.VMEM((4 * rows, vdims), bf),
        pltpu.VMEM((4, rows, depth), bf),
        pltpu.VMEM((2, rows, depth), bf),
        pltpu.VMEM((rows, depth), bf),
        pltpu.VMEM((rows, depth), bf),
        sem((10,)),
        sem((2, groups)),
        sem((2, groups)),
        sem((2, groups)),
        sem((2, groups)),
        sem((2, groups // 2)),
        sem((2, groups)),
        sem((2, groups)),
        sem((2, 3)),
        sem((2, levels)),
        sem((2, levels)),
        sem((2, levels)),
        sem((2, levels)),
        sem((2, 3)),
        sem((2, 2)),
    ]
    return pl.pallas_call(
        functools.partial(fused_kernel, heads, rope, main, rest),
        out_shape=(
            jax.ShapeDtypeStruct((rows, depth), fl),
            jax.ShapeDtypeStruct((rows, depth), fl),
        ),
        in_specs=[vmem] * len(small) + [hbm] * (1 + len(weights)),
        out_specs=(vmem, vmem),
        scratch_shapes=scratch,
        compiler_params=pltpu.CompilerParams(
            collective_id=0, has_side_effects=True, vmem_limit_bytes=62 * 1024 * 1024
        ),
    )(*small, rows_in, *weights)


def per_device(
    query_latent,
    kv_latent,
    rope_key,
    query_gain,
    kv_gain,
    query_nope_w,
    query_rope_w,
    key_up_w,
    value_up_w,
    output_w,
    expert_in,
    moe_gain,
    routes,
    route_weight,
    gate_w,
    up_w,
    down_w,
):
    tok_rows, top_count = routes.shape
    width = expert_in.shape[1]
    local = gate_w.shape[0]
    rope = rope_key.shape[1]
    heads = query_nope_w.shape[1] // NOPE
    ep_size, tp_size = lax.axis_size("ep"), lax.axis_size("tp")
    experts = local * ep_size
    capacity = max(2, 5 * tok_rows * top_count // (4 * experts))
    main = capacity // 8 * 8
    rest = capacity - main
    if not (
        tp_size == 4
        and ep_size & (ep_size - 1) == 0
        and main % 16 == 0
        and local * rest % 8 == 0
        and heads * rope == 128
        and 2 * rope == 128
        and ep_size >= 4
    ):
        return plain_device(
            query_latent,
            kv_latent,
            rope_key,
            query_gain,
            kv_gain,
            query_nope_w,
            query_rope_w,
            key_up_w,
            value_up_w,
            output_w,
            expert_in,
            moe_gain,
            routes,
            route_weight,
            gate_w,
            up_w,
            down_w,
        )
    half = rope // 2
    exponent = np.arange(half, dtype=np.float32) * np.float32(2.0) / np.float32(rope)
    freq = np.float32(1.0) / np.float32(THETA) ** exponent
    small = (
        query_latent,
        kv_latent,
        rope_key.T,
        query_gain,
        kv_gain,
        jnp.asarray(np.tile(freq, 4)[None, :]),
        moe_gain,
        routes.T,
        route_weight.T,
    )
    big = (query_nope_w, query_rope_w, key_up_w, value_up_w, output_w, gate_w, up_w, down_w)
    mixed, blend = fused(ep_size, small, expert_in, big, (heads, rope, main, rest))
    return mixed.astype(jnp.bfloat16), blend.astype(jnp.bfloat16)


def solution(mesh):
    placed = (
        P(("ep", "tp"), None),
        P(("ep", "tp"), None),
        P(("ep", "tp"), None),
        P(),
        P(),
        P(None, "tp"),
        P(None, "tp"),
        P(None, "tp"),
        P(None, "tp"),
        P("tp", None),
        P(("ep", "tp"), None),
        P(),
        P(("ep", "tp"), None),
        P(("ep", "tp"), None),
        P("ep", None, "tp"),
        P("ep", None, "tp"),
        P("ep", "tp", None),
    )
    return jax.shard_map(
        per_device,
        mesh=mesh,
        in_specs=placed,
        out_specs=(P(("ep", "tp"), None), P(("ep", "tp"), None)),
        check_vma=False,
    )
```
